128 devices in a mesh: kv: 16 (over z, y), tp: 8 (over x, core).
Axes of the slice: x: 4, y: 4, z: 4, core: 2. Of those that a mesh axis runs over, the one named last changes fastest.
Arguments:
- tokens: bfloat16 [128, 4096], P(None, 'kv'), may hold values from -8 to 8
- attn_gain: float32 [4096], P('kv'), may hold values from 0.1 to 1.9
- w_query: bfloat16 [4096, 2048], P('kv', 'tp'), may hold values from -0.09375 to 0.09375
- w_key: bfloat16 [4096, 2048], P('kv', 'tp'), may hold values from -0.09375 to 0.09375
- w_value: bfloat16 [4096, 4096], P('kv', 'tp'), may hold values from -0.09375 to 0.09375
- w_outgate: bfloat16 [4096, 4096], P('kv', 'tp'), may hold values from -0.09375 to 0.09375
- w_gates: bfloat16 [4096, 16], replicated, may hold values from -0.029907227 to 0.029907227
- forget_bias: float32 [8], replicated, may hold values from -1 to 3
- state_c: float32 [128, 8, 512, 256], P('kv', 'tp'), may hold values from -6 to 6
- state_n: float32 [128, 8, 256], P('kv', 'tp'), may hold values from -6 to 6
- state_m: float32 [128, 8], P('kv', 'tp'), may hold values from -2 to 0.5
- w_output: bfloat16 [4096, 4096], P('tp', 'kv'), may hold values from -0.09375 to 0.09375
- mlp_gain: float32 [4096], P('kv'), may hold values from 0.1 to 1.9
- w_gateff: bfloat16 [4096, 11008], P('kv', 'tp'), may hold values from -0.09375 to 0.09375
- w_upff: bfloat16 [4096, 11008], P('kv', 'tp'), may hold values from -0.09375 to 0.09375
- w_downff: bfloat16 [11008, 4096], P('tp', 'kv'), may hold values from -0.0546875 to 0.0546875
Outputs:
- mixed: bfloat16 [128, 4096], P(None, 'kv')
- new_c: float32 [128, 8, 512, 256], P('kv', 'tp')
- new_n: float32 [128, 8, 256], P('kv', 'tp')
- new_m: float32 [128, 8], P('kv', 'tp')
The draws below stay inside these ranges and needn't reach their ends.
All inputs are finite; a program needn't handle non-finite values.
Results may differ from the reference program's by a relative error of at most 0.0083.
Values may be sent and summed in bfloat16 or wider, within the bound.
No kernel may reach another device: no remote copies, remote signals or barrier semaphores. Data moves between devices by JAX's collectives and lax.ppermute only.
A program may use at most 64 MiB of HBM per device.

```python
import math
import jax
import jax.numpy as jnp
from jax import lax

D = 4096
HEADS = 8
DQK = 256
DV = 512
FF = 11008
BATCH = 128


def draw_tokens(key, part):
    key_scale = jax.random.fold_in(key, 11)
    key_values = jax.random.fold_in(key, 12)
    groups = D // 16
    scales = jnp.exp(jax.random.uniform(key_scale, (groups,), jnp.float32, math.log(0.3), math.log(3.0)))
    scales = jnp.repeat(scales, 16)
    values = jax.random.normal(key_values, (BATCH, D), jnp.float32)
    return jnp.clip(values * scales[None, :], -8.0, 8.0).astype(jnp.bfloat16)


def level_of(rng, extent, shards, smallest, largest):
    def one(position, blocks):
        heights = jax.random.uniform(jax.random.fold_in(jax.random.fold_in(rng, 6), position), (blocks,), jnp.float32, smallest / len(shards), largest / len(shards))
        return jnp.repeat(jnp.exp(heights), extent[position] // blocks).reshape((-1,) + (1,) * (len(extent) - position - 1))

    loudness = one(*shards[0])
    for cut in shards[1:]:
        loudness = loudness * one(*cut)
    return loudness


def normal_values(stream_key, extent, deviation, limit, pieces=(), held_as=jnp.bfloat16):
    entries = jax.random.normal(stream_key, extent, jnp.float32) * deviation
    if len(pieces) > 0:
        entries = level_of(stream_key, extent, pieces, -0.22, 0.18) * entries
    return jnp.clip(entries, min=-limit, max=limit).astype(held_as)


def setup_inputs(seed: int = 0) -> dict:
    streams_of = jax.random.split(jax.random.key(seed), 17)
    return {
        "tokens": draw_tokens(jax.random.fold_in(streams_of[16], 71), 0),
        "attn_gain": jnp.clip(1.0 + 0.18 * jax.random.normal(streams_of[1], (D,), jnp.float32), 0.1, 1.9),
        "w_query": normal_values(streams_of[2], (D, HEADS * DQK), D ** -0.5, 0.09375, ((0, 16), (1, 8))),
        "w_key": normal_values(streams_of[3], (D, HEADS * DQK), D ** -0.5, 0.09375, ((0, 16), (1, 8))),
        "w_value": normal_values(streams_of[4], (D, HEADS * DV), D ** -0.5, 0.09375, ((0, 16), (1, 8))),
        "w_outgate": normal_values(streams_of[5], (D, HEADS * DV), D ** -0.5, 0.09375, ((0, 16), (1, 8))),
        "w_gates": normal_values(streams_of[6], (D, 2 * HEADS), 0.0047, 0.029907227),
        "forget_bias": jnp.clip(jax.random.uniform(streams_of[7], (HEADS,), jnp.float32, -1.0, 3.0), -1.0, 3.0),
        "state_c": normal_values(streams_of[8], (BATCH, HEADS, DV, DQK), 1.0, 6.0, ((0, 16), (1, 8)), jnp.float32),
        "state_n": normal_values(streams_of[9], (BATCH, HEADS, DQK), 1.0, 6.0, ((0, 16), (1, 8)), jnp.float32),
        "state_m": jnp.clip(-2.0 + 2.5 * jax.random.uniform(streams_of[10], (BATCH, HEADS), jnp.float32) ** level_of(streams_of[10], (BATCH, HEADS), ((0, 16), (1, 8)), -0.2, 0.2), -2.0, 0.5),
        "w_output": normal_values(streams_of[11], (HEADS * DV, D), (HEADS * DV) ** -0.5, 0.09375, ((0, 8), (1, 16))),
        "mlp_gain": jnp.clip(1.0 + 0.18 * jax.random.normal(streams_of[12], (D,), jnp.float32), 0.1, 1.9),
        "w_gateff": normal_values(streams_of[13], (D, FF), D ** -0.5, 0.09375, ((0, 16), (1, 8))),
        "w_upff": normal_values(streams_of[14], (D, FF), D ** -0.5, 0.09375, ((0, 16), (1, 8))),
        "w_downff": normal_values(streams_of[15], (FF, D), FF ** -0.5, 0.0546875, ((0, 8), (1, 16))),
    }


norm_floor = 1e-05

def inverse_rms(values):
    return lax.rsqrt(lax.optimization_barrier(jnp.mean(values * values, axis=-1)) + norm_floor)

def reference(tokens, attn_gain, w_query, w_key, w_value, w_outgate, w_gates, forget_bias, state_c, state_n, state_m, w_output, mlp_gain, w_gateff, w_upff, w_downff):
    batch = tokens.shape[0]
    tok_float = tokens.astype(jnp.float32)
    scale_one = inverse_rms(tok_float)[:, None]
    normed_one = (tok_float * attn_gain).astype(jnp.bfloat16)

    def project(weight):
        return jnp.dot(normed_one, weight, preferred_element_type=jnp.float32) * scale_one
    query = (project(w_query) * DQK ** (-0.5)).reshape(batch, HEADS, DQK)
    key_vec = project(w_key).reshape(batch, HEADS, DQK)
    value = project(w_value).reshape(batch, HEADS, DV)
    out_pre = project(w_outgate).reshape(batch, HEADS, DV)
    gate_pre = project(w_gates)
    log_input = gate_pre[:, :HEADS]
    log_forget = jax.nn.log_sigmoid(gate_pre[:, HEADS:] + forget_bias)
    carried = log_forget + state_m
    new_m = jnp.maximum(carried, log_input)
    keep = jnp.exp(carried - new_m)
    admit = jnp.exp(log_input - new_m)
    new_c = keep[:, :, None, None] * state_c + admit[:, :, None, None] * value[:, :, :, None] * key_vec[:, :, None, :]
    new_n = keep[:, :, None] * state_n + admit[:, :, None] * key_vec
    numer = jnp.einsum('bhvd,bhd->bhv', new_c, query, precision=lax.Precision.HIGHEST)
    denom = jnp.maximum(jnp.abs(lax.optimization_barrier(jnp.sum(new_n * query, axis=-1))), jnp.exp(-new_m))
    head_out = (jax.nn.sigmoid(out_pre) * numer / denom[:, :, None]).reshape(batch, HEADS * DV).astype(jnp.bfloat16)
    attn_mix = jnp.dot(head_out, w_output, preferred_element_type=jnp.float32)
    middle = (tok_float + attn_mix).astype(jnp.bfloat16)
    mid_float = middle.astype(jnp.float32)
    scale_two = inverse_rms(mid_float)[:, None]
    normed_two = (mid_float * mlp_gain).astype(jnp.bfloat16)
    gate_ff = jnp.dot(normed_two, w_gateff, preferred_element_type=jnp.float32) * scale_two
    up_ff = jnp.dot(normed_two, w_upff, preferred_element_type=jnp.float32) * scale_two
    hidden_ff = (jax.nn.silu(gate_ff) * up_ff).astype(jnp.bfloat16)
    mixed = (mid_float + jnp.dot(hidden_ff, w_downff, preferred_element_type=jnp.float32)).astype(jnp.bfloat16)
    return (mixed, new_c, new_n, new_m)
```

```python
import jax
import jax.numpy as jnp
from jax import lax
from jax.sharding import Mesh, PartitionSpec as P

norm_floor = 1e-05
lanes = 128


def exchange(value, axis):
    return lax.all_to_all(value, axis, split_axis=0, concat_axis=0, tiled=True)


def sent_to_all(value, axis):
    copies = jnp.broadcast_to(value, (lax.axis_size(axis), *value.shape))
    return exchange(copies, axis)


def split_pair(value):
    high = value.astype(jnp.bfloat16)
    low = (value - high.astype(jnp.float32)).astype(jnp.bfloat16)
    return high, low


def pad_to(value, width):
    return jnp.pad(value, ((0, 0), (0, width - value.shape[1])))


def shifted(value, axis, step):
    size = lax.axis_size(axis)
    return lax.ppermute(value, axis, [(i, (i + step) % size) for i in range(size)])


def summed_over_tp(part):
    mine = part.astype(jnp.bfloat16)
    theirs = shifted(mine, "core", 1)
    pair = (mine.astype(jnp.float32) + theirs.astype(jnp.float32)).astype(jnp.bfloat16)
    size = lax.axis_size("x")
    parts = [pair] + [shifted(pair, "x", step) for step in range(1, size)]
    parts = [p.astype(jnp.float32) for p in parts]
    while len(parts) > 1:
        half = len(parts) // 2
        parts = [parts[i] + parts[i + half] for i in range(half)]
    return parts[0]


def per_device(
    tokens,
    attn_gain,
    w_query,
    w_key,
    w_value,
    w_outgate,
    w_gates,
    forget_bias,
    state_c,
    state_n,
    state_m,
    w_output,
    mlp_gain,
    w_gateff,
    w_upff,
    w_downff,
):
    kv = ("z", "y")
    kv_count = lax.axis_size(kv)
    kv_at = lax.axis_index(kv)
    tp_at = lax.axis_index(("x", "core"))
    batch = tokens.shape[0]
    width_dev = tokens.shape[1]
    width_all = width_dev * kv_count
    rows = batch // kv_count
    heads_dev = state_c.shape[1]
    heads_all = forget_bias.shape[0]
    value_size = state_c.shape[2]
    query_size = state_c.shape[3]
    query_width = heads_dev * query_size
    value_width = heads_dev * value_size
    proj_width = 2 * query_width + 2 * value_width
    gates = 2 * heads_all

    tok_float = tokens.astype(jnp.float32)
    squares_one = jnp.sum(tok_float * tok_float, axis=1, keepdims=True)
    normed_one = (tok_float * attn_gain).astype(jnp.bfloat16)
    stacked = jnp.concatenate([w_query, w_key, w_value, w_outgate], axis=1)
    proj_part = jnp.dot(normed_one, stacked, preferred_element_type=jnp.float32)
    gate_rows = lax.dynamic_slice_in_dim(w_gates, kv_at * width_dev, width_dev, 0)
    gate_part = jnp.dot(normed_one, gate_rows, preferred_element_type=jnp.float32)
    extra = jnp.concatenate([gate_part, squares_one], axis=1)
    extra_width = gates + 1
    high, low = split_pair(extra)
    sent = jnp.concatenate(
        [proj_part.astype(jnp.bfloat16), pad_to(jnp.concatenate([high, low], axis=1), lanes)], axis=1
    )
    arrived = exchange(sent.reshape(kv_count, rows, proj_width + lanes), kv)
    summed = arrived.astype(jnp.float32).sum(axis=0)
    extra_sum = (
        summed[:, proj_width : proj_width + extra_width]
        + summed[:, proj_width + extra_width : proj_width + 2 * extra_width]
    )
    scale_one = lax.rsqrt(extra_sum[:, gates] / width_all + norm_floor)[:, None]
    proj_rows = summed[:, :proj_width] * scale_one
    gate_all = extra_sum[:, :gates] * scale_one
    query = (proj_rows[:, :query_width] * query_size ** (-0.5)).reshape(rows, heads_dev, query_size)
    key_vec = proj_rows[:, query_width : 2 * query_width].reshape(rows, heads_dev, query_size)
    value = proj_rows[:, 2 * query_width : 2 * query_width + value_width].reshape(
        rows, heads_dev, value_size
    )
    out_pre = proj_rows[:, 2 * query_width + value_width :].reshape(rows, heads_dev, value_size)
    log_input = lax.dynamic_slice_in_dim(gate_all, tp_at * heads_dev, heads_dev, 1)
    forget_pre = lax.dynamic_slice_in_dim(gate_all, heads_all + tp_at * heads_dev, heads_dev, 1)
    bias_dev = lax.dynamic_slice_in_dim(forget_bias, tp_at * heads_dev, heads_dev, 0)
    log_forget = jax.nn.log_sigmoid(forget_pre + bias_dev)
    carried = log_forget + state_m
    new_m = jnp.maximum(carried, log_input)
    keep = jnp.exp(carried - new_m)
    admit = jnp.exp(log_input - new_m)
    new_c = (
        keep[:, :, None, None] * state_c
        + admit[:, :, None, None] * value[:, :, :, None] * key_vec[:, :, None, :]
    )
    new_n = keep[:, :, None] * state_n + admit[:, :, None] * key_vec
    numer = jnp.einsum("bhvd,bhd->bhv", new_c, query, precision=lax.Precision.HIGHEST)
    denom = jnp.maximum(jnp.abs(jnp.sum(new_n * query, axis=-1)), jnp.exp(-new_m))
    head_out = (
        (jax.nn.sigmoid(out_pre) * numer / denom[:, :, None])
        .reshape(rows, value_width)
        .astype(jnp.bfloat16)
    )
    heads_rows = sent_to_all(head_out, kv).reshape(batch, value_width)
    attn_part = jnp.dot(heads_rows, w_output, preferred_element_type=jnp.float32)
    attn_mix = summed_over_tp(attn_part)
    middle = (tok_float + attn_mix).astype(jnp.bfloat16)
    mid_float = middle.astype(jnp.float32)
    squares_two = jnp.sum(mid_float * mid_float, axis=1, keepdims=True)
    normed_two = (mid_float * mlp_gain).astype(jnp.bfloat16)
    gate_ff = jnp.dot(normed_two, w_gateff, preferred_element_type=jnp.float32)
    up_ff = jnp.dot(normed_two, w_upff, preferred_element_type=jnp.float32)
    hidden_dev = w_gateff.shape[1]
    hidden_pad = -(-(hidden_dev + 2) // lanes) * lanes
    high, low = split_pair(squares_two)
    sent = jnp.concatenate(
        [
            pad_to(gate_ff.astype(jnp.bfloat16), hidden_pad),
            pad_to(jnp.concatenate([up_ff.astype(jnp.bfloat16), high, low], axis=1), hidden_pad),
        ],
        axis=1,
    )
    arrived = exchange(sent.reshape(kv_count, rows, 2 * hidden_pad), kv)
    summed = arrived.astype(jnp.float32).sum(axis=0)
    at = hidden_pad + hidden_dev
    rows_two = summed[:, at : at + 1] + summed[:, at + 1 : at + 2]
    scale_two = lax.rsqrt(rows_two / width_all + norm_floor)
    hidden_ff = (
        jax.nn.silu(summed[:, :hidden_dev] * scale_two)
        * (summed[:, hidden_pad : hidden_pad + hidden_dev] * scale_two)
    ).astype(jnp.bfloat16)
    hidden_rows = sent_to_all(hidden_ff, kv).reshape(batch, hidden_dev)
    down_part = jnp.dot(hidden_rows, w_downff, preferred_element_type=jnp.float32)
    mixed = (mid_float + summed_over_tp(down_part)).astype(jnp.bfloat16)
    return (mixed, new_c, new_n, new_m)


def solution(mesh):
    kv = ("z", "y")
    tp = ("x", "core")
    cores = 2
    tp_size = mesh.shape["tp"]
    fine = Mesh(
        mesh.devices.reshape(4, mesh.shape["kv"] // 4, tp_size // cores, cores), kv + tp
    )
    placed = (
        P(None, kv),
        P(kv),
        P(kv, tp),
        P(kv, tp),
        P(kv, tp),
        P(kv, tp),
        P(),
        P(),
        P(kv, tp, None, None),
        P(kv, tp, None),
        P(kv, tp),
        P(tp, kv),
        P(kv),
        P(kv, tp),
        P(kv, tp),
        P(tp, kv),
    )
    return jax.shard_map(
        per_device,
        mesh=fine,
        in_specs=placed,
        out_specs=(P(None, kv), P(kv, tp, None, None), P(kv, tp, None), P(kv, tp)),
        check_vma=False,
    )
```

```python
import functools

import jax
import jax.numpy as jnp
from jax import lax
from jax.experimental import pallas as pl
from jax.experimental.pallas import tpu as pltpu
from jax.sharding import Mesh, PartitionSpec as P

norm_floor = 1e-05
lanes = 128
kv = ("z", "y")
tp = ("x", "core")
vmem = pl.BlockSpec(memory_space=pltpu.VMEM)
smem = pl.BlockSpec(memory_space=pltpu.SMEM)
anywhere = pl.BlockSpec(memory_space=pl.ANY)
low_at = 32
nt_dims = (((1,), (1,)), ((), ()))


def params(mib):
    return pltpu.CompilerParams(vmem_limit_bytes=mib << 20)


def cost(flops, moved):
    return pl.CostEstimate(flops=flops, bytes_accessed=moved, transcendentals=0)


def index_of(axes):
    at = 0
    for axis in axes:
        at = at * lax.axis_size(axis) + lax.axis_index(axis)
    return at


def lane_ids(shape):
    return lax.broadcasted_iota(jnp.int32, shape, len(shape) - 1)


def row_ids(shape):
    return lax.broadcasted_iota(jnp.int32, shape, 0)


def split_pair(value):
    high = value.astype(jnp.bfloat16)
    low = (value - high.astype(jnp.float32)).astype(jnp.bfloat16)
    return high, low


def exchange(value, axis):
    return lax.all_to_all(value, axis, split_axis=0, concat_axis=0, tiled=True)


def sent_to_all(value, axis):
    copies = jnp.broadcast_to(value, (lax.axis_size(axis), *value.shape))
    return exchange(copies, axis)


def shifted(value, axis, step):
    size = lax.axis_size(axis)
    return lax.ppermute(value, axis, [(i, (i + step) % size) for i in range(size)])


def over_tp(part):
    mine = part.astype(jnp.bfloat16)
    theirs = shifted(mine, "core", 1)
    pair = (mine.astype(jnp.float32) + theirs.astype(jnp.float32)).astype(jnp.bfloat16)
    return [pair] + [shifted(pair, "x", step) for step in range(1, lax.axis_size("x"))]


def in_order(terms):
    terms = [term.astype(jnp.float32) for term in terms]
    while len(terms) > 1:
        half = len(terms) // 2
        terms = [terms[i] + terms[i + half] for i in range(half)]
    return terms[0]


def project_kernel(
    tokens, gain_in, w_query, w_key, w_value, w_outgate, gates_t, sent, tok, gain, weights, gate_rows, sems
):
    width = tok.shape[1]
    gates = gates_t.shape[0]
    moves = [(tokens, tok), (gain_in, gain)]
    at = 0
    for source in (w_query, w_key, w_value, w_outgate):
        columns = source.shape[1]
        moves.append((source, weights.at[:, pl.ds(at, columns)]))
        at += columns
    mine = pl.ds(pl.multiple_of(index_of(kv) * width, width), width)
    for row in (0, low_at):
        moves.append((gates_t.at[:, mine], gate_rows.at[pl.ds(row, gates), :]))
    copies = [pltpu.make_async_copy(*move, sems.at[i]) for i, move in enumerate(moves)]
    for copy in copies:
        copy.start()
    for start, end in ((gates, low_at), (low_at + gates, lanes)):
        gate_rows[start:end, :] = jnp.zeros((end - start, width), gate_rows.dtype)
    for copy in copies[:2]:
        copy.wait()
    values = tok[...].astype(jnp.float32)
    squares = jnp.sum(values * values, axis=1, keepdims=True)
    normed = (values * gain[...]).astype(jnp.bfloat16)
    for copy in copies[2:]:
        copy.wait()
    product = jnp.dot(normed, weights[...], preferred_element_type=jnp.float32)
    sent[:, :at] = product.astype(jnp.bfloat16)
    extra = lax.dot_general(normed, gate_rows[...], nt_dims, preferred_element_type=jnp.float32)
    lane = lane_ids(extra.shape)
    extra = jnp.where((lane == gates) | (lane == low_at + gates), squares, extra)
    high, low = split_pair(extra)
    sent[:, at:] = jnp.where(lane < low_at, high.astype(jnp.float32), low.astype(jnp.float32)).astype(
        jnp.bfloat16
    )


def shorten_kernel(state, short):
    short[0] = state[0, 0].astype(jnp.bfloat16)


def cell_kernel(
    width_all, arrived, state_short, state_n, state_m, bias, sent, to_write, value_out, new_n, new_m
):
    rows = arrived.shape[1]
    value_size, query_size = state_short.shape[1:]
    proj_width = 2 * query_size + 2 * value_size
    heads = bias.shape[0]
    total = arrived[0].astype(jnp.float32)
    for i in range(1, arrived.shape[0]):
        total = total + arrived[i].astype(jnp.float32)
    extra = total[:, proj_width:]
    lane = lane_ids(extra.shape)

    def column(at):
        picked = jnp.where((lane == at) | (lane == at + low_at), extra, 0.0)
        return jnp.sum(picked, axis=1, keepdims=True)

    head = index_of(tp)
    scale = lax.rsqrt(column(2 * heads) / width_all + norm_floor)
    log_input = column(head) * scale
    forget_pre = column(heads + head) * scale + bias[head]
    log_forget = jnp.minimum(forget_pre, 0.0) - jnp.log(1.0 + jnp.exp(-jnp.abs(forget_pre)))
    square = (rows, rows)
    diagonal = row_ids(square) == lane_ids(square)
    old_m = jnp.sum(jnp.where(diagonal, jnp.broadcast_to(state_m[...], square), 0.0), axis=1, keepdims=True)
    carried = log_forget + old_m
    top = jnp.maximum(carried, log_input)
    keep = jnp.exp(carried - top)
    admit = jnp.exp(log_input - top)
    query = total[:, :query_size] * (scale * query_size ** (-0.5))
    key_in = total[:, query_size : 2 * query_size] * (scale * admit)
    value = total[:, 2 * query_size : 2 * query_size + value_size] * scale
    out_pre = total[:, 2 * query_size + value_size : proj_width] * scale
    later_n = keep * state_n[...].reshape(rows, query_size) + key_in
    normalizer = jnp.sum(later_n * query, axis=1, keepdims=True)
    denom = jnp.maximum(jnp.abs(normalizer), jnp.exp(-top))
    match = jnp.sum(key_in * query, axis=1, keepdims=True)
    q_high, q_low = split_pair(query)
    both = jnp.concatenate([q_high.astype(jnp.float32), q_low.astype(jnp.float32)], axis=0)
    row = row_ids(both.shape)
    reads = jnp.zeros((2 * rows, value_size), jnp.float32)
    for b in range(rows):
        one = jnp.where((row == b) | (row == b + rows), both, 0.0).astype(jnp.bfloat16)
        reads += lax.dot_general(one, state_short[b], nt_dims, preferred_element_type=jnp.float32)
    numer = keep * (reads[:rows] + reads[rows:]) + match * value
    head_out = numer / ((1.0 + jnp.exp(-out_pre)) * denom)
    short = head_out.astype(jnp.bfloat16)
    for i in range(sent.shape[0]):
        sent[i] = short
    to_write[:, :lanes] = jnp.broadcast_to(keep, (rows, lanes))
    to_write[:, lanes:] = key_in
    value_out[...] = value
    new_n[...] = later_n.reshape(new_n.shape)
    new_m[...] = jnp.sum(jnp.where(diagonal, jnp.broadcast_to(top, square), 0.0), axis=0, keepdims=True)


def write_kernel(to_write, value, state, new_c):
    b = pl.program_id(0)
    across = value[...].T
    picked = jnp.where(lane_ids(across.shape) == b, across, 0.0)
    down = jnp.sum(picked, axis=1, keepdims=True)
    packed = to_write[...]
    mine = jnp.sum(jnp.where(row_ids(packed.shape) == b, packed, 0.0), axis=0, keepdims=True)
    keep = mine[:, :1]
    key_in = mine[:, lanes:]
    new_c[0, 0] = keep * state[0, 0] + down * key_in


def widen_kernel(term_0, term_1, term_2, term_3, tok, gain, gate_t, up_t, sent, middle):
    attn_mix = in_order([term[...] for term in (term_0, term_1, term_2, term_3)])
    mid = (tok[...].astype(jnp.float32) + attn_mix).astype(jnp.bfloat16)
    middle[...] = mid
    mid_float = mid.astype(jnp.float32)
    squares = jnp.sum(mid_float * mid_float, axis=1, keepdims=True)
    normed = (mid_float * gain[...]).astype(jnp.bfloat16)
    hidden = gate_t.shape[0]
    half = sent.shape[1] // 2
    rest = half - hidden
    high, low = split_pair(squares)
    lane = lane_ids((tok.shape[0], rest))
    stats = jnp.where(
        lane == 0, high.astype(jnp.float32), jnp.where(lane == 1, low.astype(jnp.float32), 0.0)
    )
    for at, weight, tail in ((0, gate_t, jnp.zeros_like(stats)), (half, up_t, stats)):
        product = lax.dot_general(normed, weight[...], nt_dims, preferred_element_type=jnp.float32)
        whole = jnp.concatenate([product, tail], axis=1)
        sent[:, at : at + half] = whole.astype(jnp.bfloat16)


def per_device(
    tokens,
    attn_gain,
    w_query,
    w_key,
    w_value,
    w_outgate,
    w_gates,
    forget_bias,
    state_c,
    state_n,
    state_m,
    w_output,
    mlp_gain,
    w_gateff,
    w_upff,
    w_downff,
):
    kv_count = lax.axis_size(kv)
    batch, width_dev = tokens.shape
    width_all = width_dev * kv_count
    rows = batch // kv_count
    heads_all = forget_bias.shape[0]
    _, _, value_size, query_size = state_c.shape
    proj_width = 2 * query_size + 2 * value_size
    f32, bf16 = jnp.float32, jnp.bfloat16

    sent = pl.pallas_call(
        project_kernel,
        out_shape=jax.ShapeDtypeStruct((batch, proj_width + lanes), bf16),
        in_specs=[anywhere] * 7,
        out_specs=vmem,
        scratch_shapes=[
            pltpu.VMEM((batch, width_dev), bf16),
            pltpu.VMEM((1, width_dev), f32),
            pltpu.VMEM((width_dev, proj_width), bf16),
            pltpu.VMEM((lanes, width_dev), bf16),
            pltpu.SemaphoreType.DMA((8,)),
        ],
        cost_estimate=cost(2 * batch * width_dev * proj_width, 2 * width_dev * proj_width),
        name="project",
    )(tokens, attn_gain.reshape(1, width_dev), w_query, w_key, w_value, w_outgate, w_gates.T)
    state_short = pl.pallas_call(
        shorten_kernel,
        out_shape=jax.ShapeDtypeStruct((rows, value_size, query_size), bf16),
        grid=(rows,),
        in_specs=[pl.BlockSpec((1, 1, value_size, query_size), lambda b: (b, 0, 0, 0))],
        out_specs=pl.BlockSpec((1, value_size, query_size), lambda b: (b, 0, 0)),
        cost_estimate=cost(10**9, 6 * rows * value_size * query_size),
        name="shorten_state",
    )(state_c)
    arrived = exchange(sent.reshape(kv_count, rows, proj_width + lanes), kv)
    head_copies, to_write, value, new_n, new_m = pl.pallas_call(
        functools.partial(cell_kernel, width_all),
        out_shape=(
            jax.ShapeDtypeStruct((kv_count, rows, value_size), bf16),
            jax.ShapeDtypeStruct((rows, lanes + query_size), f32),
            jax.ShapeDtypeStruct((rows, value_size), f32),
            jax.ShapeDtypeStruct((rows, 1, query_size), f32),
            jax.ShapeDtypeStruct((1, rows), f32),
        ),
        in_specs=[vmem] * 4 + [smem],
        out_specs=[vmem] * 5,
        compiler_params=params(8),
        cost_estimate=cost(10**8, 4 * rows * value_size * query_size),
        name="cell",
    )(arrived, state_short, state_n, state_m.reshape(1, rows), forget_bias)
    block = pl.BlockSpec((1, 1, value_size, query_size), lambda b: (b, 0, 0, 0))
    new_c = pl.pallas_call(
        write_kernel,
        out_shape=jax.ShapeDtypeStruct(state_c.shape, f32),
        grid=(rows,),
        in_specs=[
            pl.BlockSpec((rows, lanes + query_size), lambda b: (0, 0)),
            pl.BlockSpec((rows, value_size), lambda b: (0, 0)),
            block,
        ],
        out_specs=block,
        cost_estimate=cost(10**9, 8 * rows * value_size * query_size),
        name="write_state",
    )(to_write, value, state_c)
    heads_rows = exchange(head_copies, kv).reshape(batch, value_size)
    attn_part = jnp.dot(heads_rows, w_output, preferred_element_type=f32)
    hidden_dev = w_gateff.shape[1]
    hidden_pad = -(-(hidden_dev + 2) // lanes) * lanes
    sent, middle = pl.pallas_call(
        widen_kernel,
        out_shape=(
            jax.ShapeDtypeStruct((batch, 2 * hidden_pad), bf16),
            jax.ShapeDtypeStruct((batch, width_dev), bf16),
        ),
        in_specs=[vmem] * 8,
        out_specs=[vmem] * 2,
        compiler_params=params(8),
        cost_estimate=cost(4 * batch * width_dev * hidden_dev, 4 * width_dev * hidden_dev),
        name="widen",
    )(
        *over_tp(attn_part),
        tokens,
        mlp_gain.reshape(1, width_dev),
        w_gateff.T,
        w_upff.T,
    )
    mid_float = middle.astype(f32)
    arrived = exchange(sent.reshape(kv_count, rows, 2 * hidden_pad), kv)
    summed = arrived.astype(jnp.float32).sum(axis=0)
    at = hidden_pad + hidden_dev
    rows_two = summed[:, at : at + 1] + summed[:, at + 1 : at + 2]
    scale_two = lax.rsqrt(rows_two / width_all + norm_floor)
    hidden_ff = (
        jax.nn.silu(summed[:, :hidden_dev] * scale_two)
        * (summed[:, hidden_pad : hidden_pad + hidden_dev] * scale_two)
    ).astype(jnp.bfloat16)
    hidden_rows = sent_to_all(hidden_ff, kv).reshape(batch, hidden_dev)
    down_part = jnp.dot(hidden_rows, w_downff, preferred_element_type=jnp.float32)
    mixed = (mid_float + in_order(over_tp(down_part))).astype(jnp.bfloat16)
    return (mixed, new_c, new_n, new_m.reshape(rows, 1))


def solution(mesh):
    cores = 2
    tp_size = mesh.shape["tp"]
    fine = Mesh(
        mesh.devices.reshape(4, mesh.shape["kv"] // 4, tp_size // cores, cores), kv + tp
    )
    placed = (
        P(None, kv),
        P(kv),
        P(kv, tp),
        P(kv, tp),
        P(kv, tp),
        P(kv, tp),
        P(),
        P(),
        P(kv, tp, None, None),
        P(kv, tp, None),
        P(kv, tp),
        P(tp, kv),
        P(kv),
        P(kv, tp),
        P(kv, tp),
        P(tp, kv),
    )
    return jax.shard_map(
        per_device,
        mesh=fine,
        in_specs=placed,
        out_specs=(P(None, kv), P(kv, tp, None, None), P(kv, tp, None), P(kv, tp)),
        check_vma=False,
    )
```

```python
import functools

import jax
import jax.numpy as jnp
from jax import lax
from jax.experimental import pallas as pl
from jax.experimental.pallas import tpu as pltpu
from jax.sharding import Mesh, PartitionSpec as P

norm_floor = 1e-05
lanes = 128
kv = ("z", "y")
tp = ("x", "core")
vmem = pl.BlockSpec(memory_space=pltpu.VMEM)
smem = pl.BlockSpec(memory_space=pltpu.SMEM)
hbm = pl.BlockSpec(memory_space=pltpu.HBM)
low_at = 32
nt_dims = (((1,), (1,)), ((), ()))


def params(mib):
    return pltpu.CompilerParams(vmem_limit_bytes=mib << 20)


def cost(flops, moved):
    return pl.CostEstimate(flops=flops, bytes_accessed=moved, transcendentals=0)


def index_of(axes):
    at = 0
    for axis in axes:
        at = at * lax.axis_size(axis) + lax.axis_index(axis)
    return at


def lane_ids(shape):
    return lax.broadcasted_iota(jnp.int32, shape, len(shape) - 1)


def row_ids(shape):
    return lax.broadcasted_iota(jnp.int32, shape, 0)


def split_pair(value):
    high = value.astype(jnp.bfloat16)
    low = (value - high.astype(jnp.float32)).astype(jnp.bfloat16)
    return high, low


def exchange(value, axis):
    return lax.all_to_all(value, axis, split_axis=0, concat_axis=0, tiled=True)


def sent_to_all(value, axis):
    copies = jnp.broadcast_to(value, (lax.axis_size(axis), *value.shape))
    return exchange(copies, axis)


def shifted(value, axis, step):
    size = lax.axis_size(axis)
    return lax.ppermute(value, axis, [(i, (i + step) % size) for i in range(size)])


def over_tp(part):
    mine = part.astype(jnp.bfloat16)
    theirs = shifted(mine, "core", 1)
    pair = (mine.astype(jnp.float32) + theirs.astype(jnp.float32)).astype(jnp.bfloat16)
    return [pair] + [shifted(pair, "x", step) for step in range(1, lax.axis_size("x"))]


def in_order(terms):
    terms = [term.astype(jnp.float32) for term in terms]
    while len(terms) > 1:
        half = len(terms) // 2
        terms = [terms[i] + terms[i + half] for i in range(half)]
    return terms[0]


def project_kernel(
    tokens, gain_in, w_query, w_key, w_value, w_outgate, gates_t, sent, tok, gain, weights, gate_rows, sems
):
    width = tok.shape[1]
    gates = gates_t.shape[0]
    moves = [(tokens, tok), (gain_in, gain)]
    at = 0
    for source in (w_query, w_key, w_value, w_outgate):
        columns = source.shape[1]
        moves.append((source, weights.at[:, pl.ds(at, columns)]))
        at += columns
    mine = pl.ds(pl.multiple_of(index_of(kv) * width, width), width)
    for row in (0, low_at):
        moves.append((gates_t.at[:, mine], gate_rows.at[pl.ds(row, gates), :]))
    copies = [pltpu.make_async_copy(*move, sems.at[i]) for i, move in enumerate(moves)]
    for copy in copies:
        copy.start()
    for start, end in ((gates, low_at), (low_at + gates, lanes)):
        gate_rows[start:end, :] = jnp.zeros((end - start, width), gate_rows.dtype)
    for copy in copies[:2]:
        copy.wait()
    values = tok[...].astype(jnp.float32)
    squares = jnp.sum(values * values, axis=1, keepdims=True)
    normed = (values * gain[...]).astype(jnp.bfloat16)
    for copy in copies[2:]:
        copy.wait()
    product = jnp.dot(normed, weights[...], preferred_element_type=jnp.float32)
    sent[:, :at] = product.astype(jnp.bfloat16)
    extra = lax.dot_general(normed, gate_rows[...], nt_dims, preferred_element_type=jnp.float32)
    lane = lane_ids(extra.shape)
    extra = jnp.where((lane == gates) | (lane == low_at + gates), squares, extra)
    high, low = split_pair(extra)
    sent[:, at:] = jnp.where(lane < low_at, high.astype(jnp.float32), low.astype(jnp.float32)).astype(
        jnp.bfloat16
    )


def shorten_kernel(state, weight, short, near, held, sems):
    count = held.shape[0]
    copies = [pltpu.make_async_copy(state.at[b, 0], held.at[b], sems.at[b]) for b in range(count)]
    copies.append(pltpu.make_async_copy(weight, near, sems.at[count]))
    for copy in copies:
        copy.start()
    for b in range(count):
        copies[b].wait()
        short[b] = held[b].astype(jnp.bfloat16)
    copies[count].wait()


def cell_kernel(
    width_all, arrived, state_short, state_n, state_m, bias, sent, to_write, value_out, new_n, new_m
):
    rows = arrived.shape[1]
    value_size, query_size = state_short.shape[1:]
    proj_width = 2 * query_size + 2 * value_size
    heads = bias.shape[0]
    total = arrived[0].astype(jnp.float32)
    for i in range(1, arrived.shape[0]):
        total = total + arrived[i].astype(jnp.float32)
    extra = total[:, proj_width:]
    lane = lane_ids(extra.shape)

    def column(at):
        picked = jnp.where((lane == at) | (lane == at + low_at), extra, 0.0)
        return jnp.sum(picked, axis=1, keepdims=True)

    head = index_of(tp)
    scale = lax.rsqrt(column(2 * heads) / width_all + norm_floor)
    log_input = column(head) * scale
    forget_pre = column(heads + head) * scale + bias[head]
    log_forget = jnp.minimum(forget_pre, 0.0) - jnp.log(1.0 + jnp.exp(-jnp.abs(forget_pre)))
    square = (rows, rows)
    diagonal = row_ids(square) == lane_ids(square)
    old_m = jnp.sum(jnp.where(diagonal, jnp.broadcast_to(state_m[...], square), 0.0), axis=1, keepdims=True)
    carried = log_forget + old_m
    top = jnp.maximum(carried, log_input)
    keep = jnp.exp(carried - top)
    admit = jnp.exp(log_input - top)
    query = total[:, :query_size] * (scale * query_size ** (-0.5))
    key_in = total[:, query_size : 2 * query_size] * (scale * admit)
    value = total[:, 2 * query_size : 2 * query_size + value_size] * scale
    out_pre = total[:, 2 * query_size + value_size : proj_width] * scale
    later_n = keep * state_n[...].reshape(rows, query_size) + key_in
    normalizer = jnp.sum(later_n * query, axis=1, keepdims=True)
    denom = jnp.maximum(jnp.abs(normalizer), jnp.exp(-top))
    match = jnp.sum(key_in * query, axis=1, keepdims=True)
    q_high, q_low = split_pair(query)
    both = jnp.concatenate([q_high.astype(jnp.float32), q_low.astype(jnp.float32)], axis=0)
    row = row_ids(both.shape)
    reads = jnp.zeros((2 * rows, value_size), jnp.float32)
    for b in range(rows):
        one = jnp.where((row == b) | (row == b + rows), both, 0.0).astype(jnp.bfloat16)
        reads += lax.dot_general(one, state_short[b], nt_dims, preferred_element_type=jnp.float32)
    numer = keep * (reads[:rows] + reads[rows:]) + match * value
    head_out = numer / ((1.0 + jnp.exp(-out_pre)) * denom)
    short = head_out.astype(jnp.bfloat16)
    for i in range(sent.shape[0]):
        sent[i] = short
    to_write[:, :lanes] = jnp.broadcast_to(keep, (rows, lanes))
    to_write[:, lanes:] = key_in
    value_out[...] = value
    new_n[...] = later_n.reshape(new_n.shape)
    new_m[...] = jnp.sum(jnp.where(diagonal, jnp.broadcast_to(top, square), 0.0), axis=0, keepdims=True)


def write_kernel(first, to_write, value, state, *refs):
    new_c, order, held, sems_in, sems_out = refs[-5:]
    order[...] = jnp.zeros_like(order)
    count = held.shape[0]
    into = [
        pltpu.make_async_copy(state.at[first + b, 0], held.at[b], sems_in.at[b])
        for b in range(count)
    ]
    out = [
        pltpu.make_async_copy(held.at[b], new_c.at[first + b, 0], sems_out.at[b])
        for b in range(count)
    ]
    for copy in into:
        copy.start()
    across = value[...].T
    for b in range(count):
        row = first + b
        down = across[:, row : row + 1]
        keep = to_write[row : row + 1, :1]
        key_in = to_write[row : row + 1, lanes:]
        into[b].wait()
        held[b] = keep * held[b] + down * key_in
        out[b].start()
    for copy in out:
        copy.wait()


def widen_kernel(
    term_0, term_1, term_2, term_3, tok, gain, gate_t, up_t, order, sent, middle
):
    attn_mix = in_order([term[...] for term in (term_0, term_1, term_2, term_3)])
    mid = (tok[...].astype(jnp.float32) + attn_mix).astype(jnp.bfloat16)
    middle[...] = mid
    mid_float = mid.astype(jnp.float32)
    squares = jnp.sum(mid_float * mid_float, axis=1, keepdims=True)
    normed = (mid_float * gain[...]).astype(jnp.bfloat16)
    hidden = gate_t.shape[0]
    half = sent.shape[1] // 2
    rest = half - hidden
    high, low = split_pair(squares)
    lane = lane_ids((tok.shape[0], rest))
    stats = jnp.where(
        lane == 0, high.astype(jnp.float32), jnp.where(lane == 1, low.astype(jnp.float32), 0.0)
    )
    for at, weight, tail in ((0, gate_t, jnp.zeros_like(stats)), (half, up_t, stats)):
        product = lax.dot_general(normed, weight[...], nt_dims, preferred_element_type=jnp.float32)
        whole = jnp.concatenate([product, tail], axis=1)
        sent[:, at : at + half] = whole.astype(jnp.bfloat16)


def per_device(
    tokens,
    attn_gain,
    w_query,
    w_key,
    w_value,
    w_outgate,
    w_gates,
    forget_bias,
    state_c,
    state_n,
    state_m,
    w_output,
    mlp_gain,
    w_gateff,
    w_upff,
    w_downff,
):
    kv_count = lax.axis_size(kv)
    batch, width_dev = tokens.shape
    width_all = width_dev * kv_count
    rows = batch // kv_count
    heads_all = forget_bias.shape[0]
    _, _, value_size, query_size = state_c.shape
    proj_width = 2 * query_size + 2 * value_size
    f32, bf16 = jnp.float32, jnp.bfloat16

    sent = pl.pallas_call(
        project_kernel,
        out_shape=jax.ShapeDtypeStruct((batch, proj_width + lanes), bf16),
        in_specs=[hbm] * 7,
        out_specs=vmem,
        scratch_shapes=[
            pltpu.VMEM((batch, width_dev), bf16),
            pltpu.VMEM((1, width_dev), f32),
            pltpu.VMEM((width_dev, proj_width), bf16),
            pltpu.VMEM((lanes, width_dev), bf16),
            pltpu.SemaphoreType.DMA((8,)),
        ],
        compiler_params=params(60),
        cost_estimate=cost(2 * batch * width_dev * proj_width, 2 * width_dev * proj_width),
        name="project",
    )(tokens, attn_gain.reshape(1, width_dev), w_query, w_key, w_value, w_outgate, w_gates.T)
    state_short, w_output_near = pl.pallas_call(
        shorten_kernel,
        out_shape=(
            jax.ShapeDtypeStruct((rows, value_size, query_size), bf16),
            jax.ShapeDtypeStruct(w_output.shape, w_output.dtype),
        ),
        in_specs=[hbm, hbm],
        out_specs=(vmem, vmem),
        scratch_shapes=[
            pltpu.VMEM((rows, value_size, query_size), f32),
            pltpu.SemaphoreType.DMA((rows + 1,)),
        ],
        compiler_params=params(49),
        cost_estimate=cost(10**9, 6 * rows * value_size * query_size),
        name="shorten_state",
    )(state_c, w_output)
    arrived = exchange(sent.reshape(kv_count, rows, proj_width + lanes), kv)
    head_copies, to_write, value, new_n, new_m = pl.pallas_call(
        functools.partial(cell_kernel, width_all),
        out_shape=(
            jax.ShapeDtypeStruct((kv_count, rows, value_size), bf16),
            jax.ShapeDtypeStruct((rows, lanes + query_size), f32),
            jax.ShapeDtypeStruct((rows, value_size), f32),
            jax.ShapeDtypeStruct((rows, 1, query_size), f32),
            jax.ShapeDtypeStruct((1, rows), f32),
        ),
        in_specs=[vmem] * 4 + [smem],
        out_specs=[vmem] * 5,
        compiler_params=params(8),
        cost_estimate=cost(10**8, 4 * rows * value_size * query_size),
        name="cell",
    )(arrived, state_short, state_n, state_m.reshape(1, rows), forget_bias)
    half_rows = rows // 2

    def written(first, *begun):
        return pl.pallas_call(
            functools.partial(write_kernel, first),
            out_shape=(
                jax.ShapeDtypeStruct(state_c.shape, f32),
                jax.ShapeDtypeStruct((8, lanes), f32),
            ),
            in_specs=[vmem, vmem, hbm] + [hbm] * len(begun),
            out_specs=(hbm, vmem),
            input_output_aliases={3: 0} if begun else {},
            scratch_shapes=[
                pltpu.VMEM((half_rows, value_size, query_size), f32),
                pltpu.SemaphoreType.DMA((half_rows,)),
                pltpu.SemaphoreType.DMA((half_rows,)),
            ],
            compiler_params=params(50),
            cost_estimate=cost(10**9, 4 * rows * value_size * query_size),
            name="write_state",
        )(to_write, value, state_c, *begun)

    begun_c, order = written(0)
    new_c, _ = written(half_rows, begun_c)
    heads_rows = exchange(head_copies, kv).reshape(batch, value_size)
    attn_part = jnp.dot(heads_rows, w_output_near, preferred_element_type=f32)
    hidden_dev = w_gateff.shape[1]
    hidden_pad = -(-(hidden_dev + 2) // lanes) * lanes
    sent, middle = pl.pallas_call(
        widen_kernel,
        out_shape=(
            jax.ShapeDtypeStruct((batch, 2 * hidden_pad), bf16),
            jax.ShapeDtypeStruct((batch, width_dev), bf16),
        ),
        in_specs=[vmem] * 9,
        out_specs=[vmem] * 2,
        compiler_params=params(8),
        cost_estimate=cost(4 * batch * width_dev * hidden_dev, 4 * width_dev * hidden_dev),
        name="widen",
    )(
        *over_tp(attn_part),
        tokens,
        mlp_gain.reshape(1, width_dev),
        w_gateff.T,
        w_upff.T,
        order,
    )
    mid_float = middle.astype(f32)
    arrived = exchange(sent.reshape(kv_count, rows, 2 * hidden_pad), kv)
    summed = arrived.astype(jnp.float32).sum(axis=0)
    at = hidden_pad + hidden_dev
    rows_two = summed[:, at : at + 1] + summed[:, at + 1 : at + 2]
    scale_two = lax.rsqrt(rows_two / width_all + norm_floor)
    hidden_ff = (
        jax.nn.silu(summed[:, :hidden_dev] * scale_two)
        * (summed[:, hidden_pad : hidden_pad + hidden_dev] * scale_two)
    ).astype(jnp.bfloat16)
    hidden_rows = sent_to_all(hidden_ff, kv).reshape(batch, hidden_dev)
    down_part = jnp.dot(hidden_rows, w_downff, preferred_element_type=jnp.float32)
    mixed = (mid_float + in_order(over_tp(down_part))).astype(jnp.bfloat16)
    return (mixed, new_c, new_n, new_m.reshape(rows, 1))


def solution(mesh):
    cores = 2
    tp_size = mesh.shape["tp"]
    fine = Mesh(
        mesh.devices.reshape(4, mesh.shape["kv"] // 4, tp_size // cores, cores), kv + tp
    )
    placed = (
        P(None, kv),
        P(kv),
        P(kv, tp),
        P(kv, tp),
        P(kv, tp),
        P(kv, tp),
        P(),
        P(),
        P(kv, tp, None, None),
        P(kv, tp, None),
        P(kv, tp),
        P(tp, kv),
        P(kv),
        P(kv, tp),
        P(kv, tp),
        P(tp, kv),
    )
    return jax.shard_map(
        per_device,
        mesh=fine,
        in_specs=placed,
        out_specs=(P(None, kv), P(kv, tp, None, None), P(kv, tp, None), P(kv, tp)),
        check_vma=False,
    )
```

```python
import functools

import jax
import jax.numpy as jnp
from jax import lax
from jax.experimental import pallas as pl
from jax.experimental.pallas import tpu as pltpu
from jax.sharding import Mesh, PartitionSpec as P


norm_floor = 1e-05
lanes = 128
kv = ("z", "y")
tp = ("x", "core")
vmem = pl.BlockSpec(memory_space=pltpu.VMEM)
hbm = pl.BlockSpec(memory_space=pltpu.HBM)
low_at = 32
nt_dims = (((1,), (1,)), ((), ()))


def params(mib):
    return pltpu.CompilerParams(vmem_limit_bytes=mib << 20)


def cost(flops, moved):
    return pl.CostEstimate(flops=flops, bytes_accessed=moved, transcendentals=0)


def index_of(axes):
    at = 0
    for axis in axes:
        at = at * lax.axis_size(axis) + lax.axis_index(axis)
    return at


def lane_ids(shape):
    return lax.broadcasted_iota(jnp.int32, shape, len(shape) - 1)


def row_ids(shape):
    return lax.broadcasted_iota(jnp.int32, shape, 0)


def split_pair(value):
    high = value.astype(jnp.bfloat16)
    low = (value - high.astype(jnp.float32)).astype(jnp.bfloat16)
    return high, low


def exchange(value, axis):
    return lax.all_to_all(value, axis, split_axis=0, concat_axis=0, tiled=True)


def sent_to_all(value, axis):
    copies = jnp.broadcast_to(value, (lax.axis_size(axis), *value.shape))
    return exchange(copies, axis)


def shifted(value, axis, step):
    size = lax.axis_size(axis)
    return lax.ppermute(value, axis, [(i, (i + step) % size) for i in range(size)])


def over_tp(part):
    mine = part.astype(jnp.bfloat16)
    theirs = shifted(mine, "core", 1)
    pair = (mine.astype(jnp.float32) + theirs.astype(jnp.float32)).astype(jnp.bfloat16)
    terms = [pair]
    for step in range(1, lax.axis_size("x")):
        terms.append(shifted(pair, "x", step))
    return terms


def in_order(terms):
    terms = [term.astype(jnp.float32) for term in terms]
    while len(terms) > 1:
        half = len(terms) // 2
        terms = [terms[i] + terms[i + half] for i in range(half)]
    return terms[0]


def project_kernel(
    tokens, gain_in, w_query, w_key, w_value, w_outgate, gates_t, sent, tok, gain, weights, gate_rows, sems
):
    width = tok.shape[1]
    gates = gates_t.shape[0]
    moves = [(tokens, tok), (gain_in, gain)]
    at = 0
    for source in (w_query, w_key, w_value, w_outgate):
        columns = source.shape[1]
        moves.append((source, weights.at[:, pl.ds(at, columns)]))
        at += columns
    mine = pl.ds(pl.multiple_of(index_of(kv) * width, width), width)
    for row in (0, low_at):
        moves.append((gates_t.at[:, mine], gate_rows.at[pl.ds(row, gates), :]))
    copies = [pltpu.make_async_copy(*move, sems.at[i]) for i, move in enumerate(moves)]
    for copy in copies:
        copy.start()
    for start, end in ((gates, low_at), (low_at + gates, lanes)):
        gate_rows[start:end, :] = jnp.zeros((end - start, width), gate_rows.dtype)
    for copy in copies[:2]:
        copy.wait()
    values = tok[...].astype(jnp.float32)
    squares = jnp.sum(values * values, axis=1, keepdims=True)
    normed = (values * gain[...]).astype(jnp.bfloat16)
    for copy in copies[2:]:
        copy.wait()
    product = jnp.dot(normed, weights[...], preferred_element_type=jnp.float32)
    sent[:, :at] = product.astype(jnp.bfloat16)
    extra = lax.dot_general(normed, gate_rows[...], nt_dims, preferred_element_type=jnp.float32)
    lane = lane_ids(extra.shape)
    extra = jnp.where((lane == gates) | (lane == low_at + gates), squares, extra)
    high, low = split_pair(extra)
    sent[:, at:] = jnp.where(lane < low_at, high.astype(jnp.float32), low.astype(jnp.float32)).astype(
        jnp.bfloat16
    )


def near_kernel(
    state, n_in, m_in, bias_in, short, packed, held, state_n, state_m, bias, sems
):
    rows, _, query_size = held.shape
    moves = [(state.at[b, 0], held.at[b]) for b in range(rows)]
    moves += [(n_in, state_n), (m_in, state_m), (bias_in, bias)]
    copies = [pltpu.make_async_copy(*move, sems.at[i]) for i, move in enumerate(moves)]
    for copy in copies:
        copy.start()
    for copy in copies[rows:]:
        copy.wait()
    square = (rows, rows)
    diagonal = row_ids(square) == lane_ids(square)
    old_m = jnp.where(diagonal, jnp.broadcast_to(state_m[...], square), 0.0)
    old_m = jnp.sum(old_m, axis=1, keepdims=True)
    mine = lane_ids(bias.shape) == index_of(tp)
    bias_here = jnp.sum(jnp.where(mine, bias[...], 0.0), axis=1, keepdims=True)
    packed[:, :query_size] = state_n[...].reshape(rows, query_size)
    packed[:, query_size:] = jnp.where(lane_ids((rows, lanes)) == 0, old_m, bias_here)
    for b in range(rows):
        copies[b].wait()
        short[b] = held[b].astype(jnp.bfloat16)


def cell_kernel(
    width_all, heads, arrived, state_short, packed, sent, to_write, value_out
):
    rows = arrived.shape[1]
    value_size, query_size = state_short.shape[1:]
    proj_width = 2 * query_size + 2 * value_size
    total = arrived[0].astype(jnp.float32)
    for i in range(1, arrived.shape[0]):
        total = total + arrived[i].astype(jnp.float32)
    extra = total[:, proj_width:]
    lane = lane_ids(extra.shape)

    def column(at):
        picked = jnp.where((lane == at) | (lane == at + low_at), extra, 0.0)
        return jnp.sum(picked, axis=1, keepdims=True)

    head = index_of(tp)
    scale = lax.rsqrt(column(2 * heads) / width_all + norm_floor)
    log_input = column(head) * scale
    old_m = packed[:, query_size : query_size + 1]
    forget_pre = column(heads + head) * scale + packed[:, query_size + 1 : query_size + 2]
    log_forget = jnp.minimum(forget_pre, 0.0) - jnp.log(1.0 + jnp.exp(-jnp.abs(forget_pre)))
    carried = log_forget + old_m
    top = jnp.maximum(carried, log_input)
    keep = jnp.exp(carried - top)
    admit = jnp.exp(log_input - top)
    query = total[:, :query_size] * (scale * query_size ** (-0.5))
    key_in = total[:, query_size : 2 * query_size] * (scale * admit)
    value = total[:, 2 * query_size : 2 * query_size + value_size] * scale
    out_pre = total[:, 2 * query_size + value_size : proj_width] * scale
    later_n = keep * packed[:, :query_size] + key_in
    normalizer = jnp.sum(later_n * query, axis=1, keepdims=True)
    denom = jnp.maximum(jnp.abs(normalizer), jnp.exp(-top))
    match = jnp.sum(key_in * query, axis=1, keepdims=True)
    q_high, q_low = split_pair(query)
    both = jnp.concatenate([q_high.astype(jnp.float32), q_low.astype(jnp.float32)], axis=0)
    row = row_ids(both.shape)
    reads = jnp.zeros((2 * rows, value_size), jnp.float32)
    for b in range(rows):
        one = jnp.where((row == b) | (row == b + rows), both, 0.0).astype(jnp.bfloat16)
        reads += lax.dot_general(one, state_short[b], nt_dims, preferred_element_type=jnp.float32)
    numer = keep * (reads[:rows] + reads[rows:]) + match * value
    head_out = numer / ((1.0 + jnp.exp(-out_pre)) * denom)
    short = head_out.astype(jnp.bfloat16)
    for i in range(sent.shape[0]):
        sent[i] = short
    lane = lane_ids((rows, lanes))
    to_write[:, :lanes] = jnp.where(lane == 0, keep, top)
    to_write[:, lanes : lanes + query_size] = key_in
    to_write[:, lanes + query_size :] = later_n
    value_out[...] = value


def write_kernel(first, to_write, value, state, *refs):
    outputs, held, sems_in, sems_out = refs[:-3], *refs[-3:]
    count, _, query_size = held.shape
    if first == 0:
        new_c, order = outputs
        order[...] = jnp.zeros_like(order)
    else:
        _, new_c, new_n, new_m = outputs
        new_n[...] = to_write[:, lanes + query_size :].reshape(new_n.shape)
        rows = to_write.shape[0]
        square = (rows, rows)
        top = jnp.broadcast_to(to_write[:, 1:2], square)
        new_m[...] = jnp.sum(
            jnp.where(row_ids(square) == lane_ids(square), top, 0.0), axis=0, keepdims=True
        )
    into = [
        pltpu.make_async_copy(state.at[first + b, 0], held.at[b], sems_in.at[b])
        for b in range(count)
    ]
    out = [
        pltpu.make_async_copy(held.at[b], new_c.at[first + b, 0], sems_out.at[b])
        for b in range(count)
    ]
    for copy in into:
        copy.start()
    across = value[...].T
    for b in range(count):
        row = first + b
        down = across[:, row : row + 1]
        keep = to_write[row : row + 1, :1]
        key_in = to_write[row : row + 1, lanes : lanes + query_size]
        into[b].wait()
        held[b] = keep * held[b] + down * key_in
        out[b].start()
    for copy in out:
        copy.wait()


def widen_kernel(
    term_0, term_1, term_2, term_3, tok, gain, gate_t, up_t, order, sent, middle
):
    attn_mix = in_order([term[...] for term in (term_0, term_1, term_2, term_3)])
    mid = (tok[...].astype(jnp.float32) + attn_mix).astype(jnp.bfloat16)
    middle[...] = mid
    mid_float = mid.astype(jnp.float32)
    squares = jnp.sum(mid_float * mid_float, axis=1, keepdims=True)
    normed = (mid_float * gain[...]).astype(jnp.bfloat16)
    hidden = gate_t.shape[0]
    half = sent.shape[1] // 2
    rest = half - hidden
    high, low = split_pair(squares)
    lane = lane_ids((tok.shape[0], rest))
    stats = jnp.where(
        lane == 0, high.astype(jnp.float32), jnp.where(lane == 1, low.astype(jnp.float32), 0.0)
    )
    for at, weight, tail in ((0, gate_t, jnp.zeros_like(stats)), (half, up_t, stats)):
        product = lax.dot_general(normed, weight[...], nt_dims, preferred_element_type=jnp.float32)
        whole = jnp.concatenate([product, tail], axis=1)
        sent[:, at : at + half] = whole.astype(jnp.bfloat16)


def per_device(
    tokens,
    attn_gain,
    w_query,
    w_key,
    w_value,
    w_outgate,
    w_gates,
    forget_bias,
    state_c,
    state_n,
    state_m,
    w_output,
    mlp_gain,
    w_gateff,
    w_upff,
    w_downff,
):
    kv_count = lax.axis_size(kv)
    batch, width_dev = tokens.shape
    width_all = width_dev * kv_count
    rows = batch // kv_count
    heads_all = forget_bias.shape[0]
    _, _, value_size, query_size = state_c.shape
    proj_width = 2 * query_size + 2 * value_size
    f32, bf16 = jnp.float32, jnp.bfloat16

    sent = pl.pallas_call(
        project_kernel,
        out_shape=jax.ShapeDtypeStruct((batch, proj_width + lanes), bf16),
        in_specs=[hbm] * 7,
        out_specs=vmem,
        scratch_shapes=[
            pltpu.VMEM((batch, width_dev), bf16),
            pltpu.VMEM((1, width_dev), f32),
            pltpu.VMEM((width_dev, proj_width), bf16),
            pltpu.VMEM((lanes, width_dev), bf16),
            pltpu.SemaphoreType.DMA((8,)),
        ],
        compiler_params=params(60),
        cost_estimate=cost(2 * batch * width_dev * proj_width, 2 * width_dev * proj_width),
        name="project",
    )(tokens, attn_gain.reshape(1, width_dev), w_query, w_key, w_value, w_outgate, w_gates.T)
    state_short, packed = pl.pallas_call(
        near_kernel,
        out_shape=(
            jax.ShapeDtypeStruct((rows, value_size, query_size), bf16),
            jax.ShapeDtypeStruct((rows, query_size + lanes), f32),
        ),
        in_specs=[hbm] * 4,
        out_specs=[vmem] * 2,
        scratch_shapes=[
            pltpu.VMEM((rows, value_size, query_size), f32),
            pltpu.VMEM(state_n.shape, f32),
            pltpu.VMEM((1, rows), f32),
            pltpu.VMEM((1, heads_all), f32),
            pltpu.SemaphoreType.DMA((rows + 3,)),
        ],
        compiler_params=params(49),
        cost_estimate=cost(10**9, 6 * rows * value_size * query_size),
        name="near",
    )(
        state_c,
        state_n,
        state_m.reshape(1, rows),
        forget_bias.reshape(1, heads_all),
    )
    arrived = exchange(sent.reshape(kv_count, rows, proj_width + lanes), kv)
    head_copies, to_write, value = pl.pallas_call(
        functools.partial(cell_kernel, width_all, heads_all),
        out_shape=(
            jax.ShapeDtypeStruct((kv_count, rows, value_size), bf16),
            jax.ShapeDtypeStruct((rows, lanes + 2 * query_size), f32),
            jax.ShapeDtypeStruct((rows, value_size), f32),
        ),
        in_specs=[vmem] * 3,
        out_specs=[vmem] * 3,
        compiler_params=params(8),
        cost_estimate=cost(10**8, 4 * rows * value_size * query_size),
        name="cell",
    )(arrived, state_short, packed)
    half_rows = rows // 2

    def written(first, extra, *begun):
        return pl.pallas_call(
            functools.partial(write_kernel, first),
            out_shape=(jax.ShapeDtypeStruct(state_c.shape, f32), *extra),
            in_specs=[vmem, vmem, hbm] + [hbm] * len(begun),
            out_specs=(hbm,) + (vmem,) * len(extra),
            input_output_aliases={3: 0} if begun else {},
            scratch_shapes=[
                pltpu.VMEM((half_rows, value_size, query_size), f32),
                pltpu.SemaphoreType.DMA((half_rows,)),
                pltpu.SemaphoreType.DMA((half_rows,)),
            ],
            compiler_params=params(50),
            cost_estimate=cost(10**9, 4 * rows * value_size * query_size),
            name="write_state",
        )(to_write, value, state_c, *begun)

    begun_c, order = written(0, (jax.ShapeDtypeStruct((8, lanes), f32),))
    new_c, new_n, new_m = written(
        half_rows,
        (jax.ShapeDtypeStruct(state_n.shape, f32), jax.ShapeDtypeStruct((1, rows), f32)),
        begun_c,
    )
    heads_rows = exchange(head_copies, kv).reshape(batch, value_size)
    attn_part = jnp.dot(heads_rows, w_output, preferred_element_type=f32)
    hidden_dev = w_gateff.shape[1]
    hidden_pad = -(-(hidden_dev + 2) // lanes) * lanes
    sent, middle = pl.pallas_call(
        widen_kernel,
        out_shape=(
            jax.ShapeDtypeStruct((batch, 2 * hidden_pad), bf16),
            jax.ShapeDtypeStruct((batch, width_dev), bf16),
        ),
        in_specs=[vmem] * 9,
        out_specs=[vmem] * 2,
        compiler_params=params(8),
        cost_estimate=cost(4 * batch * width_dev * hidden_dev, 4 * width_dev * hidden_dev),
        name="widen",
    )(
        *over_tp(attn_part),
        tokens,
        mlp_gain.reshape(1, width_dev),
        w_gateff.T,
        w_upff.T,
        order,
    )
    mid_float = middle.astype(f32)
    arrived = exchange(sent.reshape(kv_count, rows, 2 * hidden_pad), kv)
    summed = arrived.astype(jnp.float32).sum(axis=0)
    at = hidden_pad + hidden_dev
    rows_two = summed[:, at : at + 1] + summed[:, at + 1 : at + 2]
    scale_two = lax.rsqrt(rows_two / width_all + norm_floor)
    hidden_ff = (
        jax.nn.silu(summed[:, :hidden_dev] * scale_two)
        * (summed[:, hidden_pad : hidden_pad + hidden_dev] * scale_two)
    ).astype(jnp.bfloat16)
    hidden_rows = sent_to_all(hidden_ff, kv).reshape(batch, hidden_dev)
    down_part = jnp.dot(hidden_rows, w_downff, preferred_element_type=jnp.float32)
    mixed = (mid_float + in_order(over_tp(down_part))).astype(jnp.bfloat16)
    return (mixed, new_c, new_n, new_m.reshape(rows, 1))


def solution(mesh):
    cores = 2
    tp_size = mesh.shape["tp"]
    fine = Mesh(
        mesh.devices.reshape(4, mesh.shape["kv"] // 4, tp_size // cores, cores), kv + tp
    )
    placed = (
        P(None, kv),
        P(kv),
        P(kv, tp),
        P(kv, tp),
        P(kv, tp),
        P(kv, tp),
        P(),
        P(),
        P(kv, tp, None, None),
        P(kv, tp, None),
        P(kv, tp),
        P(tp, kv),
        P(kv),
        P(kv, tp),
        P(kv, tp),
        P(tp, kv),
    )
    return jax.shard_map(
        per_device,
        mesh=fine,
        in_specs=placed,
        out_specs=(P(None, kv), P(kv, tp, None, None), P(kv, tp, None), P(kv, tp)),
        check_vma=False,
    )
```

```python
import functools

import jax
import jax.numpy as jnp
from jax import lax
from jax.experimental import pallas as pl
from jax.experimental.pallas import tpu as pltpu
from jax.sharding import Mesh, PartitionSpec as P


norm_floor = 1e-05
lanes = 128
kv = ("z", "y")
tp = ("x", "core")
vmem = pl.BlockSpec(memory_space=pltpu.VMEM)
hbm = pl.BlockSpec(memory_space=pltpu.HBM)
low_at = 32
extra_rows = 16
nt_dims = (((1,), (1,)), ((), ()))


def params(mib):
    return pltpu.CompilerParams(vmem_limit_bytes=mib << 20)


def cost(flops, moved):
    return pl.CostEstimate(flops=flops, bytes_accessed=moved, transcendentals=0)


def index_of(axes):
    at = 0
    for axis in axes:
        at = at * lax.axis_size(axis) + lax.axis_index(axis)
    return at


def lane_ids(shape):
    return lax.broadcasted_iota(jnp.int32, shape, len(shape) - 1)


def row_ids(shape):
    return lax.broadcasted_iota(jnp.int32, shape, 0)


def split_pair(value):
    high = value.astype(jnp.bfloat16)
    low = (value - high.astype(jnp.float32)).astype(jnp.bfloat16)
    return high, low


def split_three(value):
    parts = []
    for _ in range(3):
        part = value.astype(jnp.bfloat16).astype(jnp.float32)
        parts.append(part)
        value = value - part
    return parts


def exchange(value, axis):
    return lax.all_to_all(value, axis, split_axis=0, concat_axis=0, tiled=True)


def sent_to_all(value, axis):
    copies = jnp.broadcast_to(value, (lax.axis_size(axis), *value.shape))
    return exchange(copies, axis)


def shifted(value, axis, step):
    size = lax.axis_size(axis)
    return lax.ppermute(value, axis, [(i, (i + step) % size) for i in range(size)])


def over_tp(part):
    mine = part.astype(jnp.bfloat16)
    theirs = shifted(mine, "core", 1)
    pair = (mine.astype(jnp.float32) + theirs.astype(jnp.float32)).astype(jnp.bfloat16)
    terms = [pair]
    for step in range(1, lax.axis_size("x")):
        terms.append(shifted(pair, "x", step))
    return terms


def in_order(terms):
    terms = [term.astype(jnp.float32) for term in terms]
    while len(terms) > 1:
        half = len(terms) // 2
        terms = [terms[i] + terms[i + half] for i in range(half)]
    return terms[0]


def project_kernel(
    tokens, gain_in, w_query, w_key, w_value, w_outgate, gates_t, sent, tok, gain, weights, gate_rows, sems
):
    width = tok.shape[1]
    gates = gates_t.shape[0]
    moves = [(tokens, tok), (gain_in, gain)]
    at = 0
    for source in (w_query, w_key, w_value, w_outgate):
        columns = source.shape[1]
        moves.append((source, weights.at[:, pl.ds(at, columns)]))
        at += columns
    mine = pl.ds(pl.multiple_of(index_of(kv) * width, width), width)
    for row in (0, low_at):
        moves.append((gates_t.at[:, mine], gate_rows.at[pl.ds(row, gates), :]))
    copies = [pltpu.make_async_copy(*move, sems.at[i]) for i, move in enumerate(moves)]
    for copy in copies:
        copy.start()
    for start, end in ((gates, low_at), (low_at + gates, lanes)):
        gate_rows[start:end, :] = jnp.zeros((end - start, width), gate_rows.dtype)
    for copy in copies[:2]:
        copy.wait()
    values = tok[...].astype(jnp.float32)
    squares = jnp.sum(values * values, axis=1, keepdims=True)
    normed = (values * gain[...]).astype(jnp.bfloat16)
    for copy in copies[2:]:
        copy.wait()
    product = jnp.dot(normed, weights[...], preferred_element_type=jnp.float32)
    sent[:, :at] = product.astype(jnp.bfloat16)
    extra = lax.dot_general(normed, gate_rows[...], nt_dims, preferred_element_type=jnp.float32)
    lane = lane_ids(extra.shape)
    extra = jnp.where((lane == gates) | (lane == low_at + gates), squares, extra)
    high, low = split_pair(extra)
    sent[:, at:] = jnp.where(lane < low_at, high.astype(jnp.float32), low.astype(jnp.float32)).astype(
        jnp.bfloat16
    )


def near_kernel(
    state, weight, n_in, m_in, bias_in, short, near, held, state_n, state_m, bias, sems
):
    rows, value_size, query_size = held.shape
    moves = [(state.at[b, 0], held.at[b]) for b in range(rows)]
    moves += [(weight, near), (n_in, state_n), (m_in, state_m), (bias_in, bias)]
    copies = [pltpu.make_async_copy(*move, sems.at[i]) for i, move in enumerate(moves)]
    for copy in copies:
        copy.start()
    for copy in copies[rows + 1 :]:
        copy.wait()
    square = (rows, rows)
    diagonal = row_ids(square) == lane_ids(square)
    old_m = jnp.where(diagonal, jnp.broadcast_to(state_m[...], square), 0.0)
    old_m = jnp.sum(old_m, axis=1, keepdims=True)
    mine = lane_ids(bias.shape) == index_of(tp)
    bias_here = jnp.sum(jnp.where(mine, bias[...], 0.0), axis=1, keepdims=True)
    row = row_ids((extra_rows, query_size))
    for b in range(rows):
        block = jnp.zeros((extra_rows, query_size), jnp.float32)
        for i, source in enumerate((state_n[b], old_m[b : b + 1], bias_here)):
            for j, part in enumerate(split_three(source)):
                block = jnp.where(row == 3 * i + j, part, block)
        short[b, value_size:] = block.astype(jnp.bfloat16)
    for b in range(rows):
        copies[b].wait()
        short[b, :value_size] = held[b].astype(jnp.bfloat16)
    copies[rows].wait()


def cell_kernel(
    width_all, heads, arrived, state_short, sent, to_write, value_out
):
    rows = arrived.shape[1]
    value_size, query_size = state_short.shape[1] - extra_rows, state_short.shape[2]
    kept = state_short[:, value_size:, :].astype(jnp.float32)
    state_n, old_m, bias = (kept[:, i] + kept[:, i + 1] + kept[:, i + 2] for i in (0, 3, 6))
    proj_width = 2 * query_size + 2 * value_size
    total = arrived[0].astype(jnp.float32)
    for i in range(1, arrived.shape[0]):
        total = total + arrived[i].astype(jnp.float32)
    extra = total[:, proj_width:]
    lane = lane_ids(extra.shape)

    def column(at):
        picked = jnp.where((lane == at) | (lane == at + low_at), extra, 0.0)
        return jnp.sum(picked, axis=1, keepdims=True)

    head = index_of(tp)
    scale = lax.rsqrt(column(2 * heads) / width_all + norm_floor)
    log_input = column(head) * scale
    forget_pre = column(heads + head) * scale + bias[:, :1]
    log_forget = jnp.minimum(forget_pre, 0.0) - jnp.log(1.0 + jnp.exp(-jnp.abs(forget_pre)))
    carried = log_forget + old_m[:, :1]
    top = jnp.maximum(carried, log_input)
    keep = jnp.exp(carried - top)
    admit = jnp.exp(log_input - top)
    query = total[:, :query_size] * (scale * query_size ** (-0.5))
    key_in = total[:, query_size : 2 * query_size] * (scale * admit)
    value = total[:, 2 * query_size : 2 * query_size + value_size] * scale
    out_pre = total[:, 2 * query_size + value_size : proj_width] * scale
    later_n = keep * state_n + key_in
    normalizer = jnp.sum(later_n * query, axis=1, keepdims=True)
    denom = jnp.maximum(jnp.abs(normalizer), jnp.exp(-top))
    match = jnp.sum(key_in * query, axis=1, keepdims=True)
    q_high, q_low = split_pair(query)
    both = jnp.concatenate([q_high.astype(jnp.float32), q_low.astype(jnp.float32)], axis=0)
    row = row_ids(both.shape)
    reads = jnp.zeros((2 * rows, value_size), jnp.float32)
    for b in range(rows):
        one = jnp.where((row == b) | (row == b + rows), both, 0.0).astype(jnp.bfloat16)
        reads += lax.dot_general(one, state_short[b, :value_size], nt_dims, preferred_element_type=jnp.float32)
    numer = keep * (reads[:rows] + reads[rows:]) + match * value
    head_out = numer / ((1.0 + jnp.exp(-out_pre)) * denom)
    short = head_out.astype(jnp.bfloat16)
    for i in range(sent.shape[0]):
        sent[i] = short
    lane = lane_ids((rows, lanes))
    to_write[:, :lanes] = jnp.where(lane == 0, keep, top)
    to_write[:, lanes : lanes + query_size] = key_in
    to_write[:, lanes + query_size :] = later_n
    value_out[...] = value


def write_kernel(first, to_write, value, state, *refs):
    outputs, held, sems_in, sems_out = refs[:-3], *refs[-3:]
    count, _, query_size = held.shape
    if first == 0:
        new_c, order = outputs
        order[...] = jnp.zeros_like(order)
    else:
        _, new_c, new_n, new_m = outputs
        new_n[...] = to_write[:, lanes + query_size :].reshape(new_n.shape)
        rows = to_write.shape[0]
        square = (rows, rows)
        top = jnp.broadcast_to(to_write[:, 1:2], square)
        new_m[...] = jnp.sum(
            jnp.where(row_ids(square) == lane_ids(square), top, 0.0), axis=0, keepdims=True
        )
    into = [
        pltpu.make_async_copy(state.at[first + b, 0], held.at[b], sems_in.at[b])
        for b in range(count)
    ]
    out = [
        pltpu.make_async_copy(held.at[b], new_c.at[first + b, 0], sems_out.at[b])
        for b in range(count)
    ]
    for copy in into:
        copy.start()
    across = value[...].T
    for b in range(count):
        row = first + b
        down = across[:, row : row + 1]
        keep = to_write[row : row + 1, :1]
        key_in = to_write[row : row + 1, lanes : lanes + query_size]
        into[b].wait()
        held[b] = keep * held[b] + down * key_in
        out[b].start()
    for copy in out:
        copy.wait()


def widen_kernel(
    term_0, term_1, term_2, term_3, tok, gain, gate_t, up_t, order, sent, middle
):
    attn_mix = in_order([term[...] for term in (term_0, term_1, term_2, term_3)])
    mid = (tok[...].astype(jnp.float32) + attn_mix).astype(jnp.bfloat16)
    middle[...] = mid
    mid_float = mid.astype(jnp.float32)
    squares = jnp.sum(mid_float * mid_float, axis=1, keepdims=True)
    normed = (mid_float * gain[...]).astype(jnp.bfloat16)
    hidden = gate_t.shape[0]
    half = sent.shape[1] // 2
    rest = half - hidden
    high, low = split_pair(squares)
    lane = lane_ids((tok.shape[0], rest))
    stats = jnp.where(
        lane == 0, high.astype(jnp.float32), jnp.where(lane == 1, low.astype(jnp.float32), 0.0)
    )
    for at, weight, tail in ((0, gate_t, jnp.zeros_like(stats)), (half, up_t, stats)):
        product = lax.dot_general(normed, weight[...], nt_dims, preferred_element_type=jnp.float32)
        whole = jnp.concatenate([product, tail], axis=1)
        sent[:, at : at + half] = whole.astype(jnp.bfloat16)


def per_device(
    tokens,
    attn_gain,
    w_query,
    w_key,
    w_value,
    w_outgate,
    w_gates,
    forget_bias,
    state_c,
    state_n,
    state_m,
    w_output,
    mlp_gain,
    w_gateff,
    w_upff,
    w_downff,
):
    kv_count = lax.axis_size(kv)
    batch, width_dev = tokens.shape
    width_all = width_dev * kv_count
    rows = batch // kv_count
    heads_all = forget_bias.shape[0]
    _, _, value_size, query_size = state_c.shape
    proj_width = 2 * query_size + 2 * value_size
    f32, bf16 = jnp.float32, jnp.bfloat16

    sent = pl.pallas_call(
        project_kernel,
        out_shape=jax.ShapeDtypeStruct((batch, proj_width + lanes), bf16),
        in_specs=[hbm] * 7,
        out_specs=vmem,
        scratch_shapes=[
            pltpu.VMEM((batch, width_dev), bf16),
            pltpu.VMEM((1, width_dev), f32),
            pltpu.VMEM((width_dev, proj_width), bf16),
            pltpu.VMEM((lanes, width_dev), bf16),
            pltpu.SemaphoreType.DMA((8,)),
        ],
        compiler_params=params(63),
        cost_estimate=cost(2 * batch * width_dev * proj_width, 2 * width_dev * proj_width),
        name="project",
    )(tokens, attn_gain.reshape(1, width_dev), w_query, w_key, w_value, w_outgate, w_gates.T)
    state_short, w_output_near = pl.pallas_call(
        near_kernel,
        out_shape=(
            jax.ShapeDtypeStruct((rows, value_size + extra_rows, query_size), bf16),
            jax.ShapeDtypeStruct(w_output.shape, w_output.dtype),
        ),
        in_specs=[hbm] * 5,
        out_specs=[vmem] * 2,
        scratch_shapes=[
            pltpu.VMEM((rows, value_size, query_size), f32),
            pltpu.VMEM(state_n.shape, f32),
            pltpu.VMEM((1, rows), f32),
            pltpu.VMEM((1, heads_all), f32),
            pltpu.SemaphoreType.DMA((rows + 4,)),
        ],
        compiler_params=params(49),
        cost_estimate=cost(10**9, 6 * rows * value_size * query_size),
        name="near",
    )(
        state_c,
        w_output,
        state_n,
        state_m.reshape(1, rows),
        forget_bias.reshape(1, heads_all),
    )
    arrived = exchange(sent.reshape(kv_count, rows, proj_width + lanes), kv)
    head_copies, to_write, value = pl.pallas_call(
        functools.partial(cell_kernel, width_all, heads_all),
        out_shape=(
            jax.ShapeDtypeStruct((kv_count, rows, value_size), bf16),
            jax.ShapeDtypeStruct((rows, lanes + 2 * query_size), f32),
            jax.ShapeDtypeStruct((rows, value_size), f32),
        ),
        in_specs=[vmem] * 2,
        out_specs=[vmem] * 3,
        compiler_params=params(8),
        cost_estimate=cost(10**8, 4 * rows * value_size * query_size),
        name="cell",
    )(arrived, state_short)
    half_rows = rows // 2

    def written(first, extra, *begun):
        return pl.pallas_call(
            functools.partial(write_kernel, first),
            out_shape=(jax.ShapeDtypeStruct(state_c.shape, f32), *extra),
            in_specs=[vmem, vmem, hbm] + [hbm] * len(begun),
            out_specs=(hbm,) + (vmem,) * len(extra),
            input_output_aliases={3: 0} if begun else {},
            scratch_shapes=[
                pltpu.VMEM((half_rows, value_size, query_size), f32),
                pltpu.SemaphoreType.DMA((half_rows,)),
                pltpu.SemaphoreType.DMA((half_rows,)),
            ],
            compiler_params=params(50),
            cost_estimate=cost(10**9, 4 * rows * value_size * query_size),
            name="write_state",
        )(to_write, value, state_c, *begun)

    begun_c, order = written(0, (jax.ShapeDtypeStruct((8, lanes), f32),))
    new_c, new_n, new_m = written(
        half_rows,
        (jax.ShapeDtypeStruct(state_n.shape, f32), jax.ShapeDtypeStruct((1, rows), f32)),
        begun_c,
    )
    heads_rows = exchange(head_copies, kv).reshape(batch, value_size)
    attn_part = jnp.dot(heads_rows, w_output_near, preferred_element_type=f32)
    hidden_dev = w_gateff.shape[1]
    hidden_pad = -(-(hidden_dev + 2) // lanes) * lanes
    sent, middle = pl.pallas_call(
        widen_kernel,
        out_shape=(
            jax.ShapeDtypeStruct((batch, 2 * hidden_pad), bf16),
            jax.ShapeDtypeStruct((batch, width_dev), bf16),
        ),
        in_specs=[vmem] * 9,
        out_specs=[vmem] * 2,
        compiler_params=params(8),
        cost_estimate=cost(4 * batch * width_dev * hidden_dev, 4 * width_dev * hidden_dev),
        name="widen",
    )(
        *over_tp(attn_part),
        tokens,
        mlp_gain.reshape(1, width_dev),
        w_gateff.T,
        w_upff.T,
        order,
    )
    mid_float = middle.astype(f32)
    arrived = exchange(sent.reshape(kv_count, rows, 2 * hidden_pad), kv)
    summed = arrived.astype(jnp.float32).sum(axis=0)
    at = hidden_pad + hidden_dev
    rows_two = summed[:, at : at + 1] + summed[:, at + 1 : at + 2]
    scale_two = lax.rsqrt(rows_two / width_all + norm_floor)
    hidden_ff = (
        jax.nn.silu(summed[:, :hidden_dev] * scale_two)
        * (summed[:, hidden_pad : hidden_pad + hidden_dev] * scale_two)
    ).astype(jnp.bfloat16)
    hidden_rows = sent_to_all(hidden_ff, kv).reshape(batch, hidden_dev)
    down_part = jnp.dot(hidden_rows, w_downff, preferred_element_type=jnp.float32)
    mixed = (mid_float + in_order(over_tp(down_part))).astype(jnp.bfloat16)
    return (mixed, new_c, new_n, new_m.reshape(rows, 1))


def solution(mesh):
    cores = 2
    tp_size = mesh.shape["tp"]
    fine = Mesh(
        mesh.devices.reshape(4, mesh.shape["kv"] // 4, tp_size // cores, cores), kv + tp
    )
    placed = (
        P(None, kv),
        P(kv),
        P(kv, tp),
        P(kv, tp),
        P(kv, tp),
        P(kv, tp),
        P(),
        P(),
        P(kv, tp, None, None),
        P(kv, tp, None),
        P(kv, tp),
        P(tp, kv),
        P(kv),
        P(kv, tp),
        P(kv, tp),
        P(tp, kv),
    )
    return jax.shard_map(
        per_device,
        mesh=fine,
        in_specs=placed,
        out_specs=(P(None, kv), P(kv, tp, None, None), P(kv, tp, None), P(kv, tp)),
        check_vma=False,
    )
```

```python
import functools

import jax
import jax.numpy as jnp
from jax import lax
from jax.experimental import pallas as pl
from jax.experimental.pallas import tpu as pltpu
from jax.sharding import Mesh, PartitionSpec as P


norm_floor = 1e-05
lanes = 128
kv = ("z", "y")
tp = ("x", "core")
vmem = pl.BlockSpec(memory_space=pltpu.VMEM)
hbm = pl.BlockSpec(memory_space=pltpu.HBM)
low_at = 32
nt_dims = (((1,), (1,)), ((), ()))


def params(mib):
    return pltpu.CompilerParams(vmem_limit_bytes=mib << 20)


def cost(flops, moved):
    return pl.CostEstimate(flops=flops, bytes_accessed=moved, transcendentals=0)


def index_of(axes):
    at = 0
    for axis in axes:
        at = at * lax.axis_size(axis) + lax.axis_index(axis)
    return at


def lane_ids(shape):
    return lax.broadcasted_iota(jnp.int32, shape, len(shape) - 1)


def row_ids(shape):
    return lax.broadcasted_iota(jnp.int32, shape, 0)


def split_pair(value):
    high = value.astype(jnp.bfloat16)
    low = (value - high.astype(jnp.float32)).astype(jnp.bfloat16)
    return high, low


def split_three(value):
    parts = []
    for _ in range(3):
        part = value.astype(jnp.bfloat16)
        parts.append(part)
        value = value - part.astype(jnp.float32)
    return parts


def exchange(value, axis):
    return lax.all_to_all(value, axis, split_axis=0, concat_axis=0, tiled=True)


def sent_to_all(value, axis):
    copies = jnp.broadcast_to(value, (lax.axis_size(axis), *value.shape))
    return exchange(copies, axis)


def shifted(value, axis, step):
    size = lax.axis_size(axis)
    return lax.ppermute(value, axis, [(i, (i + step) % size) for i in range(size)])


def over_tp(part):
    mine = part.astype(jnp.bfloat16)
    theirs = shifted(mine, "core", 1)
    pair = (mine.astype(jnp.float32) + theirs.astype(jnp.float32)).astype(jnp.bfloat16)
    terms = [pair]
    for step in range(1, lax.axis_size("x")):
        terms.append(shifted(pair, "x", step))
    return terms


def in_order(terms):
    terms = [term.astype(jnp.float32) for term in terms]
    while len(terms) > 1:
        half = len(terms) // 2
        terms = [terms[i] + terms[i + half] for i in range(half)]
    return terms[0]


def project_kernel(
    tokens, gain_in, w_query, w_key, w_value, w_outgate, gates_t, sent, tok, gain, weights, gate_rows, sems
):
    width = tok.shape[1]
    gates = gates_t.shape[0]
    moves = [(tokens, tok), (gain_in, gain)]
    at = 0
    for source in (w_query, w_key, w_value, w_outgate):
        columns = source.shape[1]
        moves.append((source, weights.at[:, pl.ds(at, columns)]))
        at += columns
    mine = pl.ds(pl.multiple_of(index_of(kv) * width, width), width)
    for row in (0, low_at):
        moves.append((gates_t.at[:, mine], gate_rows.at[pl.ds(row, gates), :]))
    copies = [pltpu.make_async_copy(*move, sems.at[i]) for i, move in enumerate(moves)]
    for copy in copies:
        copy.start()
    for start, end in ((gates, low_at), (low_at + gates, lanes)):
        gate_rows[start:end, :] = jnp.zeros((end - start, width), gate_rows.dtype)
    for copy in copies[:2]:
        copy.wait()
    values = tok[...].astype(jnp.float32)
    squares = jnp.sum(values * values, axis=1, keepdims=True)
    normed = (values * gain[...]).astype(jnp.bfloat16)
    for copy in copies[2:]:
        copy.wait()
    product = jnp.dot(normed, weights[...], preferred_element_type=jnp.float32)
    sent[:, :at] = product.astype(jnp.bfloat16)
    extra = lax.dot_general(normed, gate_rows[...], nt_dims, preferred_element_type=jnp.float32)
    lane = lane_ids(extra.shape)
    extra = jnp.where((lane == gates) | (lane == low_at + gates), squares, extra)
    high, low = split_pair(extra)
    sent[:, at:] = jnp.where(lane < low_at, high.astype(jnp.float32), low.astype(jnp.float32)).astype(
        jnp.bfloat16
    )


def near_kernel(
    state, weight, n_in, m_in, bias_in, short, near, held, state_n, state_m, bias, sems
):
    rows, value_size, query_size = held.shape
    moves = [(state.at[b, 0], held.at[b]) for b in range(rows)]
    moves += [(weight, near), (n_in, state_n), (m_in, state_m), (bias_in, bias)]
    copies = [pltpu.make_async_copy(*move, sems.at[i]) for i, move in enumerate(moves)]
    for copy in copies:
        copy.start()
    for copy in copies[rows + 1 :]:
        copy.wait()
    square = (rows, rows)
    diagonal = row_ids(square) == lane_ids(square)
    old_m = jnp.where(diagonal, jnp.broadcast_to(state_m[...], square), 0.0)
    old_m = jnp.sum(old_m, axis=1, keepdims=True)
    mine = lane_ids(bias.shape) == index_of(tp)
    bias_here = jnp.sum(jnp.where(mine, bias[...], 0.0), axis=1, keepdims=True)
    whole = (rows, query_size)
    at = rows * value_size
    for source in (
        state_n[...].reshape(whole),
        jnp.where(lane_ids(whole) < lanes, old_m, bias_here),
    ):
        for part in split_three(source):
            short[at : at + rows] = part
            at += rows
    for b in range(rows):
        copies[b].wait()
        short[b * value_size : (b + 1) * value_size] = held[b].astype(jnp.bfloat16)
    copies[rows].wait()


def cell_kernel(
    width_all, heads, arrived, state_short, sent, to_write, value_out
):
    rows = arrived.shape[1]
    query_size = state_short.shape[1]
    value_size = value_out.shape[1]
    at = rows * value_size
    kept = [
        state_short[at + i * rows : at + (i + 1) * rows].astype(jnp.float32) for i in range(6)
    ]
    state_n = kept[0] + kept[1] + kept[2]
    others = kept[3] + kept[4] + kept[5]
    proj_width = 2 * query_size + 2 * value_size
    total = arrived[0].astype(jnp.float32)
    for i in range(1, arrived.shape[0]):
        total = total + arrived[i].astype(jnp.float32)
    extra = total[:, proj_width:]
    lane = lane_ids(extra.shape)

    def column(at):
        picked = jnp.where((lane == at) | (lane == at + low_at), extra, 0.0)
        return jnp.sum(picked, axis=1, keepdims=True)

    head = index_of(tp)
    scale = lax.rsqrt(column(2 * heads) / width_all + norm_floor)
    log_input = column(head) * scale
    forget_pre = column(heads + head) * scale + others[:, lanes : lanes + 1]
    log_forget = jnp.minimum(forget_pre, 0.0) - jnp.log(1.0 + jnp.exp(-jnp.abs(forget_pre)))
    carried = log_forget + others[:, :1]
    top = jnp.maximum(carried, log_input)
    keep = jnp.exp(carried - top)
    admit = jnp.exp(log_input - top)
    query = total[:, :query_size] * (scale * query_size ** (-0.5))
    key_in = total[:, query_size : 2 * query_size] * (scale * admit)
    value = total[:, 2 * query_size : 2 * query_size + value_size] * scale
    out_pre = total[:, 2 * query_size + value_size : proj_width] * scale
    later_n = keep * state_n + key_in
    normalizer = jnp.sum(later_n * query, axis=1, keepdims=True)
    denom = jnp.maximum(jnp.abs(normalizer), jnp.exp(-top))
    match = jnp.sum(key_in * query, axis=1, keepdims=True)
    q_high, q_low = split_pair(query)
    both = jnp.concatenate([q_high.astype(jnp.float32), q_low.astype(jnp.float32)], axis=0)
    row = row_ids(both.shape)
    reads = jnp.zeros((2 * rows, value_size), jnp.float32)
    for b in range(rows):
        one = jnp.where((row == b) | (row == b + rows), both, 0.0).astype(jnp.bfloat16)
        block = state_short[b * value_size : (b + 1) * value_size]
        reads += lax.dot_general(one, block, nt_dims, preferred_element_type=jnp.float32)
    numer = keep * (reads[:rows] + reads[rows:]) + match * value
    head_out = numer / ((1.0 + jnp.exp(-out_pre)) * denom)
    short = head_out.astype(jnp.bfloat16)
    for i in range(sent.shape[0]):
        sent[i] = short
    lane = lane_ids((rows, lanes))
    to_write[:, :lanes] = jnp.where(lane == 0, keep, top)
    to_write[:, lanes : lanes + query_size] = key_in
    to_write[:, lanes + query_size :] = later_n
    value_out[...] = value


def write_kernel(to_write, value, state, new_c, new_n, new_m, held, sems_in, sems_out):
    rows, _, query_size = held.shape
    into = [pltpu.make_async_copy(state.at[b, 0], held.at[b], sems_in.at[b]) for b in range(rows)]
    out = [pltpu.make_async_copy(held.at[b], new_c.at[b, 0], sems_out.at[b]) for b in range(rows)]
    for copy in into:
        copy.start()
    new_n[...] = to_write[:, lanes + query_size :].reshape(new_n.shape)
    square = (rows, rows)
    top = jnp.broadcast_to(to_write[:, 1:2], square)
    diagonal = row_ids(square) == lane_ids(square)
    new_m[...] = jnp.sum(jnp.where(diagonal, top, 0.0), axis=0, keepdims=True)
    across = value[...].T
    for b in range(rows):
        down = across[:, b : b + 1]
        keep = to_write[b : b + 1, :1]
        key_in = to_write[b : b + 1, lanes : lanes + query_size]
        into[b].wait()
        held[b] = keep * held[b] + down * key_in
        out[b].start()
    for copy in out:
        copy.wait()


def widen_kernel(term_0, term_1, term_2, term_3, tok, gain, gate_t, up_t, sent, middle):
    attn_mix = in_order([term[...] for term in (term_0, term_1, term_2, term_3)])
    mid = (tok[...].astype(jnp.float32) + attn_mix).astype(jnp.bfloat16)
    middle[...] = mid
    mid_float = mid.astype(jnp.float32)
    squares = jnp.sum(mid_float * mid_float, axis=1, keepdims=True)
    normed = (mid_float * gain[...]).astype(jnp.bfloat16)
    hidden = gate_t.shape[0]
    half = sent.shape[1] // 2
    rest = half - hidden
    high, low = split_pair(squares)
    lane = lane_ids((tok.shape[0], rest))
    stats = jnp.where(
        lane == 0, high.astype(jnp.float32), jnp.where(lane == 1, low.astype(jnp.float32), 0.0)
    )
    for at, weight, tail in ((0, gate_t, jnp.zeros_like(stats)), (half, up_t, stats)):
        product = lax.dot_general(normed, weight[...], nt_dims, preferred_element_type=jnp.float32)
        whole = jnp.concatenate([product, tail], axis=1)
        sent[:, at : at + half] = whole.astype(jnp.bfloat16)


def per_device(
    tokens,
    attn_gain,
    w_query,
    w_key,
    w_value,
    w_outgate,
    w_gates,
    forget_bias,
    state_c,
    state_n,
    state_m,
    w_output,
    mlp_gain,
    w_gateff,
    w_upff,
    w_downff,
):
    kv_count = lax.axis_size(kv)
    batch, width_dev = tokens.shape
    width_all = width_dev * kv_count
    rows = batch // kv_count
    heads_all = forget_bias.shape[0]
    _, _, value_size, query_size = state_c.shape
    proj_width = 2 * query_size + 2 * value_size
    f32, bf16 = jnp.float32, jnp.bfloat16

    sent = pl.pallas_call(
        project_kernel,
        out_shape=jax.ShapeDtypeStruct((batch, proj_width + lanes), bf16),
        in_specs=[hbm] * 7,
        out_specs=vmem,
        scratch_shapes=[
            pltpu.VMEM((batch, width_dev), bf16),
            pltpu.VMEM((1, width_dev), f32),
            pltpu.VMEM((width_dev, proj_width), bf16),
            pltpu.VMEM((lanes, width_dev), bf16),
            pltpu.SemaphoreType.DMA((8,)),
        ],
        compiler_params=params(60),
        cost_estimate=cost(2 * batch * width_dev * proj_width, 2 * width_dev * proj_width),
        name="project",
    )(tokens, attn_gain.reshape(1, width_dev), w_query, w_key, w_value, w_outgate, w_gates.T)
    state_short, w_output_near = pl.pallas_call(
        near_kernel,
        out_shape=(
            jax.ShapeDtypeStruct((rows * (value_size + 6), query_size), bf16),
            jax.ShapeDtypeStruct(w_output.shape, w_output.dtype),
        ),
        in_specs=[hbm] * 5,
        out_specs=[vmem] * 2,
        scratch_shapes=[
            pltpu.VMEM((rows, value_size, query_size), f32),
            pltpu.VMEM(state_n.shape, f32),
            pltpu.VMEM((1, rows), f32),
            pltpu.VMEM((1, heads_all), f32),
            pltpu.SemaphoreType.DMA((rows + 4,)),
        ],
        compiler_params=params(49),
        cost_estimate=cost(10**9, 6 * rows * value_size * query_size),
        name="near",
    )(
        state_c,
        w_output,
        state_n,
        state_m.reshape(1, rows),
        forget_bias.reshape(1, heads_all),
    )
    arrived = exchange(sent.reshape(kv_count, rows, proj_width + lanes), kv)
    head_copies, to_write, value = pl.pallas_call(
        functools.partial(cell_kernel, width_all, heads_all),
        out_shape=(
            jax.ShapeDtypeStruct((kv_count, rows, value_size), bf16),
            jax.ShapeDtypeStruct((rows, lanes + 2 * query_size), f32),
            jax.ShapeDtypeStruct((rows, value_size), f32),
        ),
        in_specs=[vmem] * 2,
        out_specs=[vmem] * 3,
        compiler_params=params(8),
        cost_estimate=cost(10**10, 4 * rows * value_size * query_size),
        name="cell",
    )(arrived, state_short)
    new_c, new_n, new_m = pl.pallas_call(
        write_kernel,
        out_shape=(
            jax.ShapeDtypeStruct(state_c.shape, f32),
            jax.ShapeDtypeStruct(state_n.shape, f32),
            jax.ShapeDtypeStruct((1, rows), f32),
        ),
        in_specs=[vmem, vmem, hbm],
        out_specs=(hbm, vmem, vmem),
        scratch_shapes=[
            pltpu.VMEM((rows, value_size, query_size), f32),
            pltpu.SemaphoreType.DMA((rows,)),
            pltpu.SemaphoreType.DMA((rows,)),
        ],
        compiler_params=params(50),
        cost_estimate=cost(10**9, 8 * rows * value_size * query_size),
        name="write_state",
    )(to_write, value, state_c)
    heads_rows = exchange(head_copies, kv).reshape(batch, value_size)
    attn_part = jnp.dot(heads_rows, w_output_near, preferred_element_type=f32)
    hidden_dev = w_gateff.shape[1]
    hidden_pad = -(-(hidden_dev + 2) // lanes) * lanes
    sent, middle = pl.pallas_call(
        widen_kernel,
        out_shape=(
            jax.ShapeDtypeStruct((batch, 2 * hidden_pad), bf16),
            jax.ShapeDtypeStruct((batch, width_dev), bf16),
        ),
        in_specs=[vmem] * 8,
        out_specs=[vmem] * 2,
        compiler_params=params(8),
        cost_estimate=cost(4 * batch * width_dev * hidden_dev, 4 * width_dev * hidden_dev),
        name="widen",
    )(
        *over_tp(attn_part),
        tokens,
        mlp_gain.reshape(1, width_dev),
        w_gateff.T,
        w_upff.T,
    )
    mid_float = middle.astype(f32)
    arrived = exchange(sent.reshape(kv_count, rows, 2 * hidden_pad), kv)
    summed = arrived.astype(jnp.float32).sum(axis=0)
    at = hidden_pad + hidden_dev
    rows_two = summed[:, at : at + 1] + summed[:, at + 1 : at + 2]
    scale_two = lax.rsqrt(rows_two / width_all + norm_floor)
    hidden_ff = (
        jax.nn.silu(summed[:, :hidden_dev] * scale_two)
        * (summed[:, hidden_pad : hidden_pad + hidden_dev] * scale_two)
    ).astype(jnp.bfloat16)
    hidden_rows = sent_to_all(hidden_ff, kv).reshape(batch, hidden_dev)
    down_part = jnp.dot(hidden_rows, w_downff, preferred_element_type=jnp.float32)
    mixed = (mid_float + in_order(over_tp(down_part))).astype(jnp.bfloat16)
    return (mixed, new_c, new_n, new_m.reshape(rows, 1))


def solution(mesh):
    cores = 2
    tp_size = mesh.shape["tp"]
    fine = Mesh(
        mesh.devices.reshape(4, mesh.shape["kv"] // 4, tp_size // cores, cores), kv + tp
    )
    placed = (
        P(None, kv),
        P(kv),
        P(kv, tp),
        P(kv, tp),
        P(kv, tp),
        P(kv, tp),
        P(),
        P(),
        P(kv, tp, None, None),
        P(kv, tp, None),
        P(kv, tp),
        P(tp, kv),
        P(kv),
        P(kv, tp),
        P(kv, tp),
        P(tp, kv),
    )
    return jax.shard_map(
        per_device,
        mesh=fine,
        in_specs=placed,
        out_specs=(P(None, kv), P(kv, tp, None, None), P(kv, tp, None), P(kv, tp)),
        check_vma=False,
    )
```

```python
import functools

import jax
import jax.numpy as jnp
from jax import lax
from jax.experimental import pallas as pl
from jax.experimental.pallas import tpu as pltpu
from jax.sharding import Mesh, PartitionSpec as P


norm_floor = 1e-05
lanes = 128
kv = ("z", "y")
tp = ("x", "core")
vmem = pl.BlockSpec(memory_space=pltpu.VMEM)
hbm = pl.BlockSpec(memory_space=pltpu.HBM)
low_at = 32
nt_dims = (((1,), (1,)), ((), ()))


def params(mib):
    return pltpu.CompilerParams(vmem_limit_bytes=mib << 20)


def cost(flops, moved):
    return pl.CostEstimate(flops=flops, bytes_accessed=moved, transcendentals=0)


def index_of(axes):
    at = 0
    for axis in axes:
        at = at * lax.axis_size(axis) + lax.axis_index(axis)
    return at


def lane_ids(shape):
    return lax.broadcasted_iota(jnp.int32, shape, len(shape) - 1)


def row_ids(shape):
    return lax.broadcasted_iota(jnp.int32, shape, 0)


def split_pair(value):
    high = value.astype(jnp.bfloat16)
    low = (value - high.astype(jnp.float32)).astype(jnp.bfloat16)
    return high, low


def split_three(value):
    parts = []
    for _ in range(3):
        part = value.astype(jnp.bfloat16)
        parts.append(part)
        value = value - part.astype(jnp.float32)
    return parts


def exchange(value, axis):
    return lax.all_to_all(value, axis, split_axis=0, concat_axis=0, tiled=True)


def sent_to_all(value, axis):
    copies = jnp.broadcast_to(value, (lax.axis_size(axis), *value.shape))
    return exchange(copies, axis)


def swapped(value, axis, bits):
    return lax.ppermute(value, axis, [(i, i ^ bits) for i in range(lax.axis_size(axis))])


def over_tp(part):
    mine = part.astype(jnp.bfloat16)
    theirs = swapped(mine, "core", 1)
    pair = (mine.astype(jnp.float32) + theirs.astype(jnp.float32)).astype(jnp.bfloat16)
    terms = [pair]
    for step in range(1, lax.axis_size("x")):
        terms.append(swapped(pair, "x", step))
    return terms


def in_order(terms):
    terms = [term.astype(jnp.float32) for term in terms]
    while len(terms) > 1:
        half = len(terms) // 2
        terms = [terms[i] + terms[i + half] for i in range(half)]
    return terms[0]


def project_kernel(
    tokens, gain_in, w_query, w_key, w_value, w_outgate, gates_t, sent, tok, gain, weights, gate_rows, sems
):
    width = tok.shape[1]
    gates = gates_t.shape[0]
    moves = [(tokens, tok), (gain_in, gain)]
    at = 0
    for source in (w_query, w_key, w_value, w_outgate):
        columns = source.shape[1]
        moves.append((source, weights.at[:, pl.ds(at, columns)]))
        at += columns
    mine = pl.ds(pl.multiple_of(index_of(kv) * width, width), width)
    for row in (0, low_at):
        moves.append((gates_t.at[:, mine], gate_rows.at[pl.ds(row, gates), :]))
    copies = [pltpu.make_async_copy(*move, sems.at[i]) for i, move in enumerate(moves)]
    for copy in copies:
        copy.start()
    for start, end in ((gates, low_at), (low_at + gates, lanes)):
        gate_rows[start:end, :] = jnp.zeros((end - start, width), gate_rows.dtype)
    for copy in copies[:2]:
        copy.wait()
    values = tok[...].astype(jnp.float32)
    squares = jnp.sum(values * values, axis=1, keepdims=True)
    normed = (values * gain[...]).astype(jnp.bfloat16)
    for copy in copies[2:]:
        copy.wait()
    product = jnp.dot(normed, weights[...], preferred_element_type=jnp.float32)
    sent[:, :at] = product.astype(jnp.bfloat16)
    extra = lax.dot_general(normed, gate_rows[...], nt_dims, preferred_element_type=jnp.float32)
    lane = lane_ids(extra.shape)
    extra = jnp.where((lane == gates) | (lane == low_at + gates), squares, extra)
    high, low = split_pair(extra)
    sent[:, at:] = jnp.where(lane < low_at, high.astype(jnp.float32), low.astype(jnp.float32)).astype(
        jnp.bfloat16
    )


def near_kernel(
    state, weight, n_in, m_in, bias_in, short, near, held, state_n, state_m, bias, sems
):
    rows, value_size, query_size = held.shape
    moves = [(state.at[b, 0], held.at[b]) for b in range(rows)]
    moves += [(weight, near), (n_in, state_n), (m_in, state_m), (bias_in, bias)]
    copies = [pltpu.make_async_copy(*move, sems.at[i]) for i, move in enumerate(moves)]
    for copy in copies:
        copy.start()
    for copy in copies[rows + 1 :]:
        copy.wait()
    square = (rows, rows)
    diagonal = row_ids(square) == lane_ids(square)
    old_m = jnp.where(diagonal, jnp.broadcast_to(state_m[...], square), 0.0)
    old_m = jnp.sum(old_m, axis=1, keepdims=True)
    mine = lane_ids(bias.shape) == index_of(tp)
    bias_here = jnp.sum(jnp.where(mine, bias[...], 0.0), axis=1, keepdims=True)
    whole = (rows, query_size)
    at = rows * value_size
    for source in (
        state_n[...].reshape(whole),
        jnp.where(lane_ids(whole) < lanes, old_m, bias_here),
    ):
        for part in split_three(source):
            short[at : at + rows] = part
            at += rows
    for b in range(rows):
        copies[b].wait()
        short[b * value_size : (b + 1) * value_size] = held[b].astype(jnp.bfloat16)
    copies[rows].wait()


def cell_kernel(
    width_all, heads, arrived, state_short, sent, to_write, value_out
):
    rows = arrived.shape[1]
    query_size = state_short.shape[1]
    value_size = value_out.shape[1]
    at = rows * value_size
    kept = [
        state_short[at + i * rows : at + (i + 1) * rows].astype(jnp.float32) for i in range(6)
    ]
    state_n = kept[0] + kept[1] + kept[2]
    others = kept[3] + kept[4] + kept[5]
    proj_width = 2 * query_size + 2 * value_size
    total = arrived[0].astype(jnp.float32)
    for i in range(1, arrived.shape[0]):
        total = total + arrived[i].astype(jnp.float32)
    extra = total[:, proj_width:]
    lane = lane_ids(extra.shape)

    def column(at):
        picked = jnp.where((lane == at) | (lane == at + low_at), extra, 0.0)
        return jnp.sum(picked, axis=1, keepdims=True)

    head = index_of(tp)
    scale = lax.rsqrt(column(2 * heads) / width_all + norm_floor)
    log_input = column(head) * scale
    forget_pre = column(heads + head) * scale + others[:, lanes : lanes + 1]
    log_forget = jnp.minimum(forget_pre, 0.0) - jnp.log(1.0 + jnp.exp(-jnp.abs(forget_pre)))
    carried = log_forget + others[:, :1]
    top = jnp.maximum(carried, log_input)
    keep = jnp.exp(carried - top)
    admit = jnp.exp(log_input - top)
    query = total[:, :query_size] * (scale * query_size ** (-0.5))
    key_in = total[:, query_size : 2 * query_size] * (scale * admit)
    value = total[:, 2 * query_size : 2 * query_size + value_size] * scale
    out_pre = total[:, 2 * query_size + value_size : proj_width] * scale
    later_n = keep * state_n + key_in
    normalizer = jnp.sum(later_n * query, axis=1, keepdims=True)
    denom = jnp.maximum(jnp.abs(normalizer), jnp.exp(-top))
    match = jnp.sum(key_in * query, axis=1, keepdims=True)
    q_high, q_low = split_pair(query)
    both = jnp.concatenate([q_high.astype(jnp.float32), q_low.astype(jnp.float32)], axis=0)
    row = row_ids(both.shape)
    reads = jnp.zeros((2 * rows, value_size), jnp.float32)
    for b in range(rows):
        one = jnp.where((row == b) | (row == b + rows), both, 0.0).astype(jnp.bfloat16)
        block = state_short[b * value_size : (b + 1) * value_size]
        reads += lax.dot_general(one, block, nt_dims, preferred_element_type=jnp.float32)
    numer = keep * (reads[:rows] + reads[rows:]) + match * value
    head_out = numer / ((1.0 + jnp.exp(-out_pre)) * denom)
    short = head_out.astype(jnp.bfloat16)
    for i in range(sent.shape[0]):
        sent[i] = short
    lane = lane_ids((rows, lanes))
    to_write[:, :lanes] = jnp.where(lane == 0, keep, top)
    to_write[:, lanes : lanes + query_size] = key_in
    to_write[:, lanes + query_size :] = later_n
    value_out[...] = value


def write_kernel(first, to_write, value, state, *refs):
    outputs, held, sems_in, sems_out = refs[:-3], *refs[-3:]
    count, _, query_size = held.shape
    if first == 0:
        new_c, order = outputs
        order[...] = jnp.zeros_like(order)
    else:
        _, new_c, new_n, new_m = outputs
        new_n[...] = to_write[:, lanes + query_size :].reshape(new_n.shape)
        rows = to_write.shape[0]
        square = (rows, rows)
        top = jnp.broadcast_to(to_write[:, 1:2], square)
        new_m[...] = jnp.sum(
            jnp.where(row_ids(square) == lane_ids(square), top, 0.0), axis=0, keepdims=True
        )
    into = [
        pltpu.make_async_copy(state.at[first + b, 0], held.at[b], sems_in.at[b])
        for b in range(count)
    ]
    out = [
        pltpu.make_async_copy(held.at[b], new_c.at[first + b, 0], sems_out.at[b])
        for b in range(count)
    ]
    for copy in into:
        copy.start()
    across = value[...].T
    for b in range(count):
        row = first + b
        down = across[:, row : row + 1]
        keep = to_write[row : row + 1, :1]
        key_in = to_write[row : row + 1, lanes : lanes + query_size]
        into[b].wait()
        held[b] = keep * held[b] + down * key_in
        out[b].start()
    for copy in out:
        copy.wait()


def widen_kernel(
    term_0, term_1, term_2, term_3, tok, gain, gate_t, up_t, order, sent, middle
):
    attn_mix = in_order([term[...] for term in (term_0, term_1, term_2, term_3)])
    mid = (tok[...].astype(jnp.float32) + attn_mix).astype(jnp.bfloat16)
    middle[...] = mid
    mid_float = mid.astype(jnp.float32)
    squares = jnp.sum(mid_float * mid_float, axis=1, keepdims=True)
    normed = (mid_float * gain[...]).astype(jnp.bfloat16)
    hidden = gate_t.shape[0]
    half = sent.shape[1] // 2
    rest = half - hidden
    high, low = split_pair(squares)
    lane = lane_ids((tok.shape[0], rest))
    stats = jnp.where(
        lane == 0, high.astype(jnp.float32), jnp.where(lane == 1, low.astype(jnp.float32), 0.0)
    )
    for at, weight, tail in ((0, gate_t, jnp.zeros_like(stats)), (half, up_t, stats)):
        product = lax.dot_general(normed, weight[...], nt_dims, preferred_element_type=jnp.float32)
        whole = jnp.concatenate([product, tail], axis=1)
        sent[:, at : at + half] = whole.astype(jnp.bfloat16)


def per_device(
    tokens,
    attn_gain,
    w_query,
    w_key,
    w_value,
    w_outgate,
    w_gates,
    forget_bias,
    state_c,
    state_n,
    state_m,
    w_output,
    mlp_gain,
    w_gateff,
    w_upff,
    w_downff,
):
    kv_count = lax.axis_size(kv)
    batch, width_dev = tokens.shape
    width_all = width_dev * kv_count
    rows = batch // kv_count
    heads_all = forget_bias.shape[0]
    _, _, value_size, query_size = state_c.shape
    proj_width = 2 * query_size + 2 * value_size
    f32, bf16 = jnp.float32, jnp.bfloat16

    sent = pl.pallas_call(
        project_kernel,
        out_shape=jax.ShapeDtypeStruct((batch, proj_width + lanes), bf16),
        in_specs=[hbm] * 7,
        out_specs=vmem,
        scratch_shapes=[
            pltpu.VMEM((batch, width_dev), bf16),
            pltpu.VMEM((1, width_dev), f32),
            pltpu.VMEM((width_dev, proj_width), bf16),
            pltpu.VMEM((lanes, width_dev), bf16),
            pltpu.SemaphoreType.DMA((8,)),
        ],
        compiler_params=params(60),
        cost_estimate=cost(2 * batch * width_dev * proj_width, 2 * width_dev * proj_width),
        name="project",
    )(tokens, attn_gain.reshape(1, width_dev), w_query, w_key, w_value, w_outgate, w_gates.T)
    state_short, w_output_near = pl.pallas_call(
        near_kernel,
        out_shape=(
            jax.ShapeDtypeStruct((rows * (value_size + 6), query_size), bf16),
            jax.ShapeDtypeStruct(w_output.shape, w_output.dtype),
        ),
        in_specs=[hbm] * 5,
        out_specs=[vmem] * 2,
        scratch_shapes=[
            pltpu.VMEM((rows, value_size, query_size), f32),
            pltpu.VMEM(state_n.shape, f32),
            pltpu.VMEM((1, rows), f32),
            pltpu.VMEM((1, heads_all), f32),
            pltpu.SemaphoreType.DMA((rows + 4,)),
        ],
        compiler_params=params(49),
        cost_estimate=cost(10**9, 6 * rows * value_size * query_size),
        name="near",
    )(
        state_c,
        w_output,
        state_n,
        state_m.reshape(1, rows),
        forget_bias.reshape(1, heads_all),
    )
    arrived = exchange(sent.reshape(kv_count, rows, proj_width + lanes), kv)
    head_copies, to_write, value = pl.pallas_call(
        functools.partial(cell_kernel, width_all, heads_all),
        out_shape=(
            jax.ShapeDtypeStruct((kv_count, rows, value_size), bf16),
            jax.ShapeDtypeStruct((rows, lanes + 2 * query_size), f32),
            jax.ShapeDtypeStruct((rows, value_size), f32),
        ),
        in_specs=[vmem] * 2,
        out_specs=[vmem] * 3,
        compiler_params=params(8),
        cost_estimate=cost(10**10, 4 * rows * value_size * query_size),
        name="cell",
    )(arrived, state_short)
    half_rows = rows // 2

    def written(first, extra, *begun):
        return pl.pallas_call(
            functools.partial(write_kernel, first),
            out_shape=(jax.ShapeDtypeStruct(state_c.shape, f32), *extra),
            in_specs=[vmem, vmem, hbm] + [hbm] * len(begun),
            out_specs=(hbm,) + (vmem,) * len(extra),
            input_output_aliases={3: 0} if begun else {},
            scratch_shapes=[
                pltpu.VMEM((half_rows, value_size, query_size), f32),
                pltpu.SemaphoreType.DMA((half_rows,)),
                pltpu.SemaphoreType.DMA((half_rows,)),
            ],
            compiler_params=params(50),
            cost_estimate=cost(10**9, 4 * rows * value_size * query_size),
            name="write_state",
        )(to_write, value, state_c, *begun)

    begun_c, order = written(0, (jax.ShapeDtypeStruct((8, lanes), f32),))
    new_c, new_n, new_m = written(
        half_rows,
        (jax.ShapeDtypeStruct(state_n.shape, f32), jax.ShapeDtypeStruct((1, rows), f32)),
        begun_c,
    )
    heads_rows = exchange(head_copies, kv).reshape(batch, value_size)
    attn_part = jnp.dot(heads_rows, w_output_near, preferred_element_type=f32)
    hidden_dev = w_gateff.shape[1]
    hidden_pad = -(-(hidden_dev + 2) // lanes) * lanes
    sent, middle = pl.pallas_call(
        widen_kernel,
        out_shape=(
            jax.ShapeDtypeStruct((batch, 2 * hidden_pad), bf16),
            jax.ShapeDtypeStruct((batch, width_dev), bf16),
        ),
        in_specs=[vmem] * 9,
        out_specs=[vmem] * 2,
        compiler_params=params(8),
        cost_estimate=cost(4 * batch * width_dev * hidden_dev, 4 * width_dev * hidden_dev),
        name="widen",
    )(
        *over_tp(attn_part),
        tokens,
        mlp_gain.reshape(1, width_dev),
        w_gateff.T,
        w_upff.T,
        order,
    )
    mid_float = middle.astype(f32)
    arrived = exchange(sent.reshape(kv_count, rows, 2 * hidden_pad), kv)
    summed = arrived.astype(jnp.float32).sum(axis=0)
    at = hidden_pad + hidden_dev
    rows_two = summed[:, at : at + 1] + summed[:, at + 1 : at + 2]
    scale_two = lax.rsqrt(rows_two / width_all + norm_floor)
    hidden_ff = (
        jax.nn.silu(summed[:, :hidden_dev] * scale_two)
        * (summed[:, hidden_pad : hidden_pad + hidden_dev] * scale_two)
    ).astype(jnp.bfloat16)
    hidden_rows = sent_to_all(hidden_ff, kv).reshape(batch, hidden_dev)
    down_part = jnp.dot(hidden_rows, w_downff, preferred_element_type=jnp.float32)
    mixed = (mid_float + in_order(over_tp(down_part))).astype(jnp.bfloat16)
    return (mixed, new_c, new_n, new_m.reshape(rows, 1))


def solution(mesh):
    cores = 2
    tp_size = mesh.shape["tp"]
    fine = Mesh(
        mesh.devices.reshape(4, mesh.shape["kv"] // 4, tp_size // cores, cores), kv + tp
    )
    placed = (
        P(None, kv),
        P(kv),
        P(kv, tp),
        P(kv, tp),
        P(kv, tp),
        P(kv, tp),
        P(),
        P(),
        P(kv, tp, None, None),
        P(kv, tp, None),
        P(kv, tp),
        P(tp, kv),
        P(kv),
        P(kv, tp),
        P(kv, tp),
        P(tp, kv),
    )
    return jax.shard_map(
        per_device,
        mesh=fine,
        in_specs=placed,
        out_specs=(P(None, kv), P(kv, tp, None, None), P(kv, tp, None), P(kv, tp)),
        check_vma=False,
    )
```

```python
import functools

import jax
import jax.numpy as jnp
from jax import lax
from jax.experimental import pallas as pl
from jax.experimental.pallas import tpu as pltpu
from jax.sharding import Mesh, PartitionSpec as P


norm_floor = 1e-05
lanes = 128
kv = ("z", "y")
tp = ("x", "core")
vmem = pl.BlockSpec(memory_space=pltpu.VMEM)
hbm = pl.BlockSpec(memory_space=pltpu.HBM)
low_at = 32
nt_dims = (((1,), (1,)), ((), ()))


def params(mib):
    return pltpu.CompilerParams(vmem_limit_bytes=mib << 20)


def cost(flops, moved):
    return pl.CostEstimate(flops=flops, bytes_accessed=moved, transcendentals=0)


def index_of(axes):
    at = 0
    for axis in axes:
        at = at * lax.axis_size(axis) + lax.axis_index(axis)
    return at


def lane_ids(shape):
    return lax.broadcasted_iota(jnp.int32, shape, len(shape) - 1)


def row_ids(shape):
    return lax.broadcasted_iota(jnp.int32, shape, 0)


def split_pair(value):
    high = value.astype(jnp.bfloat16)
    low = (value - high.astype(jnp.float32)).astype(jnp.bfloat16)
    return high, low


def split_three(value):
    parts = []
    for _ in range(3):
        part = value.astype(jnp.bfloat16)
        parts.append(part)
        value = value - part.astype(jnp.float32)
    return parts


def exchange(value, axis):
    return lax.all_to_all(value, axis, split_axis=0, concat_axis=0, tiled=True)


def swapped(value, axis, bits):
    return lax.ppermute(value, axis, [(i, i ^ bits) for i in range(lax.axis_size(axis))])


def over_tp(part):
    mine = part.astype(jnp.bfloat16)
    theirs = swapped(mine, "core", 1)
    pair = (mine.astype(jnp.float32) + theirs.astype(jnp.float32)).astype(jnp.bfloat16)
    terms = [pair]
    for step in range(1, lax.axis_size("x")):
        terms.append(swapped(pair, "x", step))
    return terms


def in_order(terms):
    terms = [term.astype(jnp.float32) for term in terms]
    while len(terms) > 1:
        half = len(terms) // 2
        terms = [terms[i] + terms[i + half] for i in range(half)]
    return terms[0]


def project_kernel(
    tokens,
    gain_in,
    w_query,
    w_key,
    w_value,
    w_outgate,
    gates_t,
    sent,
    tok,
    gain,
    weights,
    gate_rows,
    held,
    sems,
    out_sems,
):
    width = tok.shape[1]
    gates = gates_t.shape[0]
    moves = [(tokens, tok), (gain_in, gain)]
    mine = pl.ds(pl.multiple_of(index_of(kv) * width, width), width)
    for row in (0, low_at):
        moves.append((gates_t.at[:, mine], gate_rows.at[pl.ds(row, gates), :]))
    spans = []
    at = 0
    for source in (w_query, w_key, w_value, w_outgate):
        span = pl.ds(at, source.shape[1])
        moves.append((source, weights.at[:, span]))
        spans.append(span)
        at += source.shape[1]
    spans.append(pl.ds(at, lanes))
    copies = [pltpu.make_async_copy(*move, sems.at[i]) for i, move in enumerate(moves)]
    for copy in copies:
        copy.start()
    away = [
        pltpu.make_async_copy(held.at[:, span], sent.at[:, span], out_sems.at[i])
        for i, span in enumerate(spans)
    ]
    for start, end in ((gates, low_at), (low_at + gates, lanes)):
        gate_rows[start:end, :] = jnp.zeros((end - start, width), gate_rows.dtype)
    for copy in copies[:2]:
        copy.wait()
    values = tok[...].astype(jnp.float32)
    squares = jnp.sum(values * values, axis=1, keepdims=True)
    normed = (values * gain[...]).astype(jnp.bfloat16)
    for copy in copies[2:4]:
        copy.wait()
    extra = lax.dot_general(normed, gate_rows[...], nt_dims, preferred_element_type=jnp.float32)
    lane = lane_ids(extra.shape)
    extra = jnp.where((lane == gates) | (lane == low_at + gates), squares, extra)
    high, low = split_pair(extra)
    held[:, at:] = jnp.where(lane < low_at, high.astype(jnp.float32), low.astype(jnp.float32)).astype(
        jnp.bfloat16
    )
    away[4].start()
    for copy, span, leave in zip(copies[4:], spans, away):
        copy.wait()
        product = jnp.dot(normed, weights[:, span], preferred_element_type=jnp.float32)
        held[:, span] = product.astype(jnp.bfloat16)
        leave.start()
    for leave in away:
        leave.wait()


def near_kernel(
    state, weight, n_in, m_in, bias_in, short, near, held, state_n, state_m, bias, sems
):
    rows, value_size, query_size = held.shape
    moves = [(state.at[b, 0], held.at[b]) for b in range(rows)]
    moves += [(weight, near), (n_in, state_n), (m_in, state_m), (bias_in, bias)]
    copies = [pltpu.make_async_copy(*move, sems.at[i]) for i, move in enumerate(moves)]
    for copy in copies:
        copy.start()
    for copy in copies[rows + 1 :]:
        copy.wait()
    square = (rows, rows)
    diagonal = row_ids(square) == lane_ids(square)
    old_m = jnp.where(diagonal, jnp.broadcast_to(state_m[...], square), 0.0)
    old_m = jnp.sum(old_m, axis=1, keepdims=True)
    mine = lane_ids(bias.shape) == index_of(tp)
    bias_here = jnp.sum(jnp.where(mine, bias[...], 0.0), axis=1, keepdims=True)
    whole = (rows, query_size)
    at = rows * value_size
    for source in (
        state_n[...].reshape(whole),
        jnp.where(lane_ids(whole) < lanes, old_m, bias_here),
    ):
        for part in split_three(source):
            short[at : at + rows] = part
            at += rows
    for b in range(rows):
        copies[b].wait()
        short[b * value_size : (b + 1) * value_size] = held[b].astype(jnp.bfloat16)
    copies[rows].wait()


def cell_kernel(
    width_all, heads, arrived, state_short, sent, to_write, value_out
):
    rows = arrived.shape[1]
    query_size = state_short.shape[1]
    value_size = value_out.shape[1]
    at = rows * value_size
    kept = [
        state_short[at + i * rows : at + (i + 1) * rows].astype(jnp.float32) for i in range(6)
    ]
    state_n = kept[0] + kept[1] + kept[2]
    others = kept[3] + kept[4] + kept[5]
    proj_width = 2 * query_size + 2 * value_size
    total = arrived[0].astype(jnp.float32)
    for i in range(1, arrived.shape[0]):
        total = total + arrived[i].astype(jnp.float32)
    extra = total[:, proj_width:]
    lane = lane_ids(extra.shape)

    def column(at):
        picked = jnp.where((lane == at) | (lane == at + low_at), extra, 0.0)
        return jnp.sum(picked, axis=1, keepdims=True)

    head = index_of(tp)
    scale = lax.rsqrt(column(2 * heads) / width_all + norm_floor)
    log_input = column(head) * scale
    forget_pre = column(heads + head) * scale + others[:, lanes : lanes + 1]
    log_forget = jnp.minimum(forget_pre, 0.0) - jnp.log(1.0 + jnp.exp(-jnp.abs(forget_pre)))
    carried = log_forget + others[:, :1]
    top = jnp.maximum(carried, log_input)
    keep = jnp.exp(carried - top)
    admit = jnp.exp(log_input - top)
    query = total[:, :query_size] * (scale * query_size ** (-0.5))
    key_in = total[:, query_size : 2 * query_size] * (scale * admit)
    value = total[:, 2 * query_size : 2 * query_size + value_size] * scale
    out_pre = total[:, 2 * query_size + value_size : proj_width] * scale
    later_n = keep * state_n + key_in
    normalizer = jnp.sum(later_n * query, axis=1, keepdims=True)
    denom = jnp.maximum(jnp.abs(normalizer), jnp.exp(-top))
    match = jnp.sum(key_in * query, axis=1, keepdims=True)
    q_high, q_low = split_pair(query)
    both = jnp.concatenate([q_high.astype(jnp.float32), q_low.astype(jnp.float32)], axis=0)
    row = row_ids(both.shape)
    reads = jnp.zeros((2 * rows, value_size), jnp.float32)
    for b in range(rows):
        one = jnp.where((row == b) | (row == b + rows), both, 0.0).astype(jnp.bfloat16)
        block = state_short[b * value_size : (b + 1) * value_size]
        reads += lax.dot_general(one, block, nt_dims, preferred_element_type=jnp.float32)
    numer = keep * (reads[:rows] + reads[rows:]) + match * value
    head_out = numer / ((1.0 + jnp.exp(-out_pre)) * denom)
    short = head_out.astype(jnp.bfloat16)
    for i in range(sent.shape[0]):
        sent[i] = short
    lane = lane_ids((rows, lanes))
    to_write[:, :lanes] = jnp.where(lane == 0, keep, top)
    to_write[:, lanes : lanes + query_size] = key_in
    to_write[:, lanes + query_size :] = later_n
    value_out[...] = value


def write_kernel(first, to_write, value, state, *refs):
    if first == 0:
        new_c, order, held, sems_in, sems_out = refs
        order[...] = jnp.zeros_like(order)
    else:
        _, new_c, new_n, new_m, held, sems_in, sems_out, held_n, held_m = refs
    count, _, query_size = held.shape
    into = [
        pltpu.make_async_copy(state.at[first + b, 0], held.at[b], sems_in.at[b])
        for b in range(count)
    ]
    out = [
        pltpu.make_async_copy(held.at[b], new_c.at[first + b, 0], sems_out.at[b])
        for b in range(count)
    ]
    for copy in into:
        copy.start()
    if first > 0:
        held_n[...] = to_write[:, lanes + query_size :].reshape(held_n.shape)
        rows = to_write.shape[0]
        square = (rows, rows)
        top = jnp.broadcast_to(to_write[:, 1:2], square)
        held_m[...] = jnp.sum(
            jnp.where(row_ids(square) == lane_ids(square), top, 0.0), axis=0, keepdims=True
        )
        out.append(pltpu.make_async_copy(held_n, new_n, sems_out.at[count]))
        out.append(pltpu.make_async_copy(held_m, new_m, sems_out.at[count + 1]))
        for copy in out[count:]:
            copy.start()
    across = value[...].T
    for b in range(count):
        row = first + b
        down = across[:, row : row + 1]
        keep = to_write[row : row + 1, :1]
        key_in = to_write[row : row + 1, lanes : lanes + query_size]
        into[b].wait()
        held[b] = keep * held[b] + down * key_in
        out[b].start()
    for copy in out:
        copy.wait()


def widen_kernel(
    term_0, term_1, term_2, term_3, tok, gain, gate_t, up_t, order, sent, middle
):
    attn_mix = in_order([term[...] for term in (term_0, term_1, term_2, term_3)])
    mid = (tok[...].astype(jnp.float32) + attn_mix).astype(jnp.bfloat16)
    middle[...] = mid
    mid_float = mid.astype(jnp.float32)
    squares = jnp.sum(mid_float * mid_float, axis=1, keepdims=True)
    normed = (mid_float * gain[...]).astype(jnp.bfloat16)
    hidden = gate_t.shape[0]
    half = sent.shape[1] // 2
    rest = half - hidden
    high, low = split_pair(squares)
    lane = lane_ids((tok.shape[0], rest))
    stats = jnp.where(
        lane == 0, high.astype(jnp.float32), jnp.where(lane == 1, low.astype(jnp.float32), 0.0)
    )
    for at, weight, tail in ((0, gate_t, jnp.zeros_like(stats)), (half, up_t, stats)):
        product = lax.dot_general(normed, weight[...], nt_dims, preferred_element_type=jnp.float32)
        whole = jnp.concatenate([product, tail], axis=1)
        sent[:, at : at + half] = whole.astype(jnp.bfloat16)


def hidden_kernel(width_all, hidden, arrived, sent):
    half = arrived.shape[2] // 2
    total = arrived[0].astype(jnp.float32)
    for i in range(1, arrived.shape[0]):
        total = total + arrived[i].astype(jnp.float32)
    at = half + hidden
    last = total[:, 2 * half - lanes :]
    lane = lane_ids(last.shape) - (at - (2 * half - lanes))
    squares = jnp.sum(jnp.where((lane == 0) | (lane == 1), last, 0.0), axis=1, keepdims=True)
    scale = lax.rsqrt(squares / width_all + norm_floor)
    gate = total[:, :half] * scale
    up = total[:, half:] * scale
    short = (gate / (1.0 + jnp.exp(-gate)) * up).astype(jnp.bfloat16)[:, :hidden]
    for i in range(sent.shape[0]):
        sent[i] = short


def per_device(
    tokens,
    attn_gain,
    w_query,
    w_key,
    w_value,
    w_outgate,
    w_gates,
    forget_bias,
    state_c,
    state_n,
    state_m,
    w_output,
    mlp_gain,
    w_gateff,
    w_upff,
    w_downff,
):
    kv_count = lax.axis_size(kv)
    batch, width_dev = tokens.shape
    width_all = width_dev * kv_count
    rows = batch // kv_count
    heads_all = forget_bias.shape[0]
    _, _, value_size, query_size = state_c.shape
    proj_width = 2 * query_size + 2 * value_size
    f32, bf16 = jnp.float32, jnp.bfloat16

    sent = pl.pallas_call(
        project_kernel,
        out_shape=jax.ShapeDtypeStruct((batch, proj_width + lanes), bf16),
        in_specs=[hbm] * 7,
        out_specs=hbm,
        scratch_shapes=[
            pltpu.VMEM((batch, width_dev), bf16),
            pltpu.VMEM((1, width_dev), f32),
            pltpu.VMEM((width_dev, proj_width), bf16),
            pltpu.VMEM((lanes, width_dev), bf16),
            pltpu.VMEM((batch, proj_width + lanes), bf16),
            pltpu.SemaphoreType.DMA((8,)),
            pltpu.SemaphoreType.DMA((5,)),
        ],
        compiler_params=params(60),
        cost_estimate=cost(2 * batch * width_dev * proj_width, 2 * width_dev * proj_width),
        name="project",
    )(tokens, attn_gain.reshape(1, width_dev), w_query, w_key, w_value, w_outgate, w_gates.T)
    state_short, w_output_near = pl.pallas_call(
        near_kernel,
        out_shape=(
            jax.ShapeDtypeStruct((rows * (value_size + 6), query_size), bf16),
            jax.ShapeDtypeStruct(w_output.shape, w_output.dtype),
        ),
        in_specs=[hbm] * 5,
        out_specs=[vmem] * 2,
        scratch_shapes=[
            pltpu.VMEM((rows, value_size, query_size), f32),
            pltpu.VMEM(state_n.shape, f32),
            pltpu.VMEM((1, rows), f32),
            pltpu.VMEM((1, heads_all), f32),
            pltpu.SemaphoreType.DMA((rows + 4,)),
        ],
        compiler_params=params(49),
        cost_estimate=cost(10**9, 6 * rows * value_size * query_size),
        name="near",
    )(
        state_c,
        w_output,
        state_n,
        state_m.reshape(1, rows),
        forget_bias.reshape(1, heads_all),
    )
    arrived = exchange(sent.reshape(kv_count, rows, proj_width + lanes), kv)
    head_copies, to_write, value = pl.pallas_call(
        functools.partial(cell_kernel, width_all, heads_all),
        out_shape=(
            jax.ShapeDtypeStruct((kv_count, rows, value_size), bf16),
            jax.ShapeDtypeStruct((rows, lanes + 2 * query_size), f32),
            jax.ShapeDtypeStruct((rows, value_size), f32),
        ),
        in_specs=[vmem] * 2,
        out_specs=[vmem] * 3,
        compiler_params=params(8),
        cost_estimate=cost(10**10, 4 * rows * value_size * query_size),
        name="cell",
    )(arrived, state_short)
    half_rows = rows // 2

    def written(first, extra, spec, scratch, *begun):
        return pl.pallas_call(
            functools.partial(write_kernel, first),
            out_shape=(jax.ShapeDtypeStruct(state_c.shape, f32), *extra),
            in_specs=[vmem, vmem, hbm] + [hbm] * len(begun),
            out_specs=(hbm,) + (spec,) * len(extra),
            input_output_aliases={3: 0} if begun else {},
            scratch_shapes=[
                pltpu.VMEM((half_rows, value_size, query_size), f32),
                pltpu.SemaphoreType.DMA((half_rows,)),
                pltpu.SemaphoreType.DMA((half_rows + len(scratch),)),
                *scratch,
            ],
            compiler_params=params(50),
            cost_estimate=cost(10**9, 4 * rows * value_size * query_size),
            name="write_state",
        )(to_write, value, state_c, *begun)

    begun_c, order = written(0, (jax.ShapeDtypeStruct((8, lanes), f32),), vmem, ())
    new_c, new_n, new_m = written(
        half_rows,
        (jax.ShapeDtypeStruct(state_n.shape, f32), jax.ShapeDtypeStruct((1, rows), f32)),
        hbm,
        (pltpu.VMEM(state_n.shape, f32), pltpu.VMEM((1, rows), f32)),
        begun_c,
    )
    heads_rows = exchange(head_copies, kv).reshape(batch, value_size)
    attn_part = jnp.dot(heads_rows, w_output_near, preferred_element_type=f32)
    hidden_dev = w_gateff.shape[1]
    hidden_pad = -(-(hidden_dev + 2) // lanes) * lanes
    sent, middle = pl.pallas_call(
        widen_kernel,
        out_shape=(
            jax.ShapeDtypeStruct((batch, 2 * hidden_pad), bf16),
            jax.ShapeDtypeStruct((batch, width_dev), bf16),
        ),
        in_specs=[vmem] * 9,
        out_specs=[vmem] * 2,
        compiler_params=params(8),
        cost_estimate=cost(4 * batch * width_dev * hidden_dev, 4 * width_dev * hidden_dev),
        name="widen",
    )(
        *over_tp(attn_part),
        tokens,
        mlp_gain.reshape(1, width_dev),
        w_gateff.T,
        w_upff.T,
        order,
    )
    mid_float = middle.astype(f32)
    arrived = exchange(sent.reshape(kv_count, rows, 2 * hidden_pad), kv)
    hidden_copies = pl.pallas_call(
        functools.partial(hidden_kernel, width_all, hidden_dev),
        out_shape=jax.ShapeDtypeStruct((kv_count, rows, hidden_dev), bf16),
        in_specs=[vmem],
        out_specs=vmem,
        compiler_params=params(8),
        cost_estimate=cost(10**6, 4 * kv_count * rows * hidden_pad),
        name="hidden",
    )(arrived)
    hidden_rows = exchange(hidden_copies, kv).reshape(batch, hidden_dev)
    down_part = jnp.dot(hidden_rows, w_downff, preferred_element_type=jnp.float32)
    mixed = (mid_float + in_order(over_tp(down_part))).astype(jnp.bfloat16)
    return (mixed, new_c, new_n, new_m.reshape(rows, 1))


def solution(mesh):
    cores = 2
    tp_size = mesh.shape["tp"]
    fine = Mesh(
        mesh.devices.reshape(4, mesh.shape["kv"] // 4, tp_size // cores, cores), kv + tp
    )
    placed = (
        P(None, kv),
        P(kv),
        P(kv, tp),
        P(kv, tp),
        P(kv, tp),
        P(kv, tp),
        P(),
        P(),
        P(kv, tp, None, None),
        P(kv, tp, None),
        P(kv, tp),
        P(tp, kv),
        P(kv),
        P(kv, tp),
        P(kv, tp),
        P(tp, kv),
    )
    return jax.shard_map(
        per_device,
        mesh=fine,
        in_specs=placed,
        out_specs=(P(None, kv), P(kv, tp, None, None), P(kv, tp, None), P(kv, tp)),
        check_vma=False,
    )
```

```python
import functools

import jax
import jax.numpy as jnp
from jax import lax
from jax.experimental import pallas as pl
from jax.experimental.pallas import tpu as pltpu
from jax.sharding import Mesh, PartitionSpec as P


norm_floor = 1e-05
lanes = 128
kv = ("z", "y")
tp = ("x", "core")
vmem = pl.BlockSpec(memory_space=pltpu.VMEM)
hbm = pl.BlockSpec(memory_space=pltpu.HBM)
low_at = 32
nt_dims = (((1,), (1,)), ((), ()))


def params(mib):
    return pltpu.CompilerParams(vmem_limit_bytes=mib << 20)


def cost(flops, moved):
    return pl.CostEstimate(flops=flops, bytes_accessed=moved, transcendentals=0)


def index_of(axes):
    at = 0
    for axis in axes:
        at = at * lax.axis_size(axis) + lax.axis_index(axis)
    return at


def lane_ids(shape):
    return lax.broadcasted_iota(jnp.int32, shape, len(shape) - 1)


def row_ids(shape):
    return lax.broadcasted_iota(jnp.int32, shape, 0)


def split_pair(value):
    high = value.astype(jnp.bfloat16)
    low = (value - high.astype(jnp.float32)).astype(jnp.bfloat16)
    return high, low


def split_three(value):
    parts = []
    for _ in range(3):
        part = value.astype(jnp.bfloat16)
        parts.append(part)
        value = value - part.astype(jnp.float32)
    return parts


def exchange(value, axis):
    return lax.all_to_all(value, axis, split_axis=0, concat_axis=0, tiled=True)


def swapped(value, axis, bits):
    return lax.ppermute(value, axis, [(i, i ^ bits) for i in range(lax.axis_size(axis))])


def over_tp(part):
    mine = part.astype(jnp.bfloat16)
    theirs = swapped(mine, "core", 1)
    pair = (mine.astype(jnp.float32) + theirs.astype(jnp.float32)).astype(jnp.bfloat16)
    terms = [pair]
    for step in range(1, lax.axis_size("x")):
        terms.append(swapped(pair, "x", step))
    return terms


def in_order(terms):
    terms = [term.astype(jnp.float32) for term in terms]
    while len(terms) > 1:
        half = len(terms) // 2
        terms = [terms[i] + terms[i + half] for i in range(half)]
    return terms[0]


def project_kernel(
    tokens, gain_in, w_query, w_key, w_value, w_outgate, gates_t, sent, tok, gain, weights, gate_rows, sems
):
    width = tok.shape[1]
    gates = gates_t.shape[0]
    moves = [(tokens, tok), (gain_in, gain)]
    at = 0
    for source in (w_query, w_key, w_value, w_outgate):
        columns = source.shape[1]
        moves.append((source, weights.at[:, pl.ds(at, columns)]))
        at += columns
    mine = pl.ds(pl.multiple_of(index_of(kv) * width, width), width)
    for row in (0, low_at):
        moves.append((gates_t.at[:, mine], gate_rows.at[pl.ds(row, gates), :]))
    copies = [pltpu.make_async_copy(*move, sems.at[i]) for i, move in enumerate(moves)]
    for copy in copies:
        copy.start()
    for start, end in ((gates, low_at), (low_at + gates, lanes)):
        gate_rows[start:end, :] = jnp.zeros((end - start, width), gate_rows.dtype)
    for copy in copies[:2]:
        copy.wait()
    values = tok[...].astype(jnp.float32)
    squares = jnp.sum(values * values, axis=1, keepdims=True)
    normed = (values * gain[...]).astype(jnp.bfloat16)
    for copy in copies[2:]:
        copy.wait()
    product = jnp.dot(normed, weights[...], preferred_element_type=jnp.float32)
    sent[:, :at] = product.astype(jnp.bfloat16)
    extra = lax.dot_general(normed, gate_rows[...], nt_dims, preferred_element_type=jnp.float32)
    lane = lane_ids(extra.shape)
    extra = jnp.where((lane == gates) | (lane == low_at + gates), squares, extra)
    high, low = split_pair(extra)
    sent[:, at:] = jnp.where(lane < low_at, high.astype(jnp.float32), low.astype(jnp.float32)).astype(
        jnp.bfloat16
    )


def near_kernel(
    state, weight, n_in, m_in, bias_in, short, near, held, state_n, state_m, bias, sems
):
    rows, value_size, query_size = held.shape
    moves = [(state.at[b, 0], held.at[b]) for b in range(rows)]
    moves += [(weight, near), (n_in, state_n), (m_in, state_m), (bias_in, bias)]
    copies = [pltpu.make_async_copy(*move, sems.at[i]) for i, move in enumerate(moves)]
    for copy in copies:
        copy.start()
    for copy in copies[rows + 1 :]:
        copy.wait()
    square = (rows, rows)
    diagonal = row_ids(square) == lane_ids(square)
    old_m = jnp.where(diagonal, jnp.broadcast_to(state_m[...], square), 0.0)
    old_m = jnp.sum(old_m, axis=1, keepdims=True)
    mine = lane_ids(bias.shape) == index_of(tp)
    bias_here = jnp.sum(jnp.where(mine, bias[...], 0.0), axis=1, keepdims=True)
    whole = (rows, query_size)
    at = rows * value_size
    for source in (
        state_n[...].reshape(whole),
        jnp.where(lane_ids(whole) < lanes, old_m, bias_here),
    ):
        for part in split_three(source):
            short[at : at + rows] = part
            at += rows
    for b in range(rows):
        copies[b].wait()
        short[b * value_size : (b + 1) * value_size] = held[b].astype(jnp.bfloat16)
    copies[rows].wait()


def cell_kernel(
    width_all, heads, arrived, state_short, sent, to_write, value_out
):
    rows = arrived.shape[1]
    query_size = state_short.shape[1]
    value_size = value_out.shape[1]
    at = rows * value_size
    kept = [
        state_short[at + i * rows : at + (i + 1) * rows].astype(jnp.float32) for i in range(6)
    ]
    state_n = kept[0] + kept[1] + kept[2]
    others = kept[3] + kept[4] + kept[5]
    proj_width = 2 * query_size + 2 * value_size
    total = arrived[0].astype(jnp.float32)
    for i in range(1, arrived.shape[0]):
        total = total + arrived[i].astype(jnp.float32)
    extra = total[:, proj_width:]
    lane = lane_ids(extra.shape)

    def column(at):
        picked = jnp.where((lane == at) | (lane == at + low_at), extra, 0.0)
        return jnp.sum(picked, axis=1, keepdims=True)

    head = index_of(tp)
    scale = lax.rsqrt(column(2 * heads) / width_all + norm_floor)
    log_input = column(head) * scale
    forget_pre = column(heads + head) * scale + others[:, lanes : lanes + 1]
    log_forget = jnp.minimum(forget_pre, 0.0) - jnp.log(1.0 + jnp.exp(-jnp.abs(forget_pre)))
    carried = log_forget + others[:, :1]
    top = jnp.maximum(carried, log_input)
    keep = jnp.exp(carried - top)
    admit = jnp.exp(log_input - top)
    query = total[:, :query_size] * (scale * query_size ** (-0.5))
    key_in = total[:, query_size : 2 * query_size] * (scale * admit)
    value = total[:, 2 * query_size : 2 * query_size + value_size] * scale
    out_pre = total[:, 2 * query_size + value_size : proj_width] * scale
    later_n = keep * state_n + key_in
    normalizer = jnp.sum(later_n * query, axis=1, keepdims=True)
    denom = jnp.maximum(jnp.abs(normalizer), jnp.exp(-top))
    match = jnp.sum(key_in * query, axis=1, keepdims=True)
    q_high, q_low = split_pair(query)
    both = jnp.concatenate([q_high.astype(jnp.float32), q_low.astype(jnp.float32)], axis=0)
    row = row_ids(both.shape)
    reads = jnp.zeros((2 * rows, value_size), jnp.float32)
    for b in range(rows):
        one = jnp.where((row == b) | (row == b + rows), both, 0.0).astype(jnp.bfloat16)
        block = state_short[b * value_size : (b + 1) * value_size]
        reads += lax.dot_general(one, block, nt_dims, preferred_element_type=jnp.float32)
    numer = keep * (reads[:rows] + reads[rows:]) + match * value
    head_out = numer / ((1.0 + jnp.exp(-out_pre)) * denom)
    short = head_out.astype(jnp.bfloat16)
    for i in range(sent.shape[0]):
        sent[i] = short
    lane = lane_ids((rows, lanes))
    to_write[:, :lanes] = jnp.where(lane == 0, keep, top)
    to_write[:, lanes : lanes + query_size] = key_in
    to_write[:, lanes + query_size :] = later_n
    value_out[...] = value


def write_kernel(first, to_write, value, state, *refs):
    if first == 0:
        new_c, order, held, sems_in, sems_out = refs
        order[...] = jnp.zeros_like(order)
    else:
        _, new_c, new_n, new_m, held, sems_in, sems_out, held_n, held_m = refs
    count, _, query_size = held.shape
    into = [
        pltpu.make_async_copy(state.at[first + b, 0], held.at[b], sems_in.at[b])
        for b in range(count)
    ]
    out = [
        pltpu.make_async_copy(held.at[b], new_c.at[first + b, 0], sems_out.at[b])
        for b in range(count)
    ]
    for copy in into:
        copy.start()
    if first > 0:
        held_n[...] = to_write[:, lanes + query_size :].reshape(held_n.shape)
        rows = to_write.shape[0]
        square = (rows, rows)
        top = jnp.broadcast_to(to_write[:, 1:2], square)
        held_m[...] = jnp.sum(
            jnp.where(row_ids(square) == lane_ids(square), top, 0.0), axis=0, keepdims=True
        )
        out.append(pltpu.make_async_copy(held_n, new_n, sems_out.at[count]))
        out.append(pltpu.make_async_copy(held_m, new_m, sems_out.at[count + 1]))
        for copy in out[count:]:
            copy.start()
    across = value[...].T
    for b in range(count):
        row = first + b
        down = across[:, row : row + 1]
        keep = to_write[row : row + 1, :1]
        key_in = to_write[row : row + 1, lanes : lanes + query_size]
        into[b].wait()
        held[b] = keep * held[b] + down * key_in
        out[b].start()
    for copy in out:
        copy.wait()


def widen_kernel(
    term_0, term_1, term_2, term_3, tok, gain, gate_t, up_t, order, sent, middle
):
    attn_mix = in_order([term[...] for term in (term_0, term_1, term_2, term_3)])
    mid = (tok[...].astype(jnp.float32) + attn_mix).astype(jnp.bfloat16)
    middle[...] = mid
    mid_float = mid.astype(jnp.float32)
    squares = jnp.sum(mid_float * mid_float, axis=1, keepdims=True)
    normed = (mid_float * gain[...]).astype(jnp.bfloat16)
    hidden = gate_t.shape[0]
    half = sent.shape[1] // 2
    rest = half - hidden
    high, low = split_pair(squares)
    lane = lane_ids((tok.shape[0], rest))
    stats = jnp.where(
        lane == 0, high.astype(jnp.float32), jnp.where(lane == 1, low.astype(jnp.float32), 0.0)
    )
    for at, weight, tail in ((0, gate_t, jnp.zeros_like(stats)), (half, up_t, stats)):
        product = lax.dot_general(normed, weight[...], nt_dims, preferred_element_type=jnp.float32)
        whole = jnp.concatenate([product, tail], axis=1)
        sent[:, at : at + half] = whole.astype(jnp.bfloat16)


def hidden_kernel(width_all, hidden, arrived, sent):
    half = arrived.shape[2] // 2
    total = arrived[0].astype(jnp.float32)
    for i in range(1, arrived.shape[0]):
        total = total + arrived[i].astype(jnp.float32)
    at = half + hidden
    last = total[:, 2 * half - lanes :]
    lane = lane_ids(last.shape) - (at - (2 * half - lanes))
    squares = jnp.sum(jnp.where((lane == 0) | (lane == 1), last, 0.0), axis=1, keepdims=True)
    scale = lax.rsqrt(squares / width_all + norm_floor)
    gate = total[:, :half] * scale
    up = total[:, half:] * scale
    short = (gate / (1.0 + jnp.exp(-gate)) * up).astype(jnp.bfloat16)[:, :hidden]
    for i in range(sent.shape[0]):
        sent[i] = short


def per_device(
    tokens,
    attn_gain,
    w_query,
    w_key,
    w_value,
    w_outgate,
    w_gates,
    forget_bias,
    state_c,
    state_n,
    state_m,
    w_output,
    mlp_gain,
    w_gateff,
    w_upff,
    w_downff,
):
    kv_count = lax.axis_size(kv)
    batch, width_dev = tokens.shape
    width_all = width_dev * kv_count
    rows = batch // kv_count
    heads_all = forget_bias.shape[0]
    _, _, value_size, query_size = state_c.shape
    proj_width = 2 * query_size + 2 * value_size
    f32, bf16 = jnp.float32, jnp.bfloat16

    sent = pl.pallas_call(
        project_kernel,
        out_shape=jax.ShapeDtypeStruct((batch, proj_width + lanes), bf16),
        in_specs=[hbm] * 7,
        out_specs=vmem,
        scratch_shapes=[
            pltpu.VMEM((batch, width_dev), bf16),
            pltpu.VMEM((1, width_dev), f32),
            pltpu.VMEM((width_dev, proj_width), bf16),
            pltpu.VMEM((lanes, width_dev), bf16),
            pltpu.SemaphoreType.DMA((8,)),
        ],
        compiler_params=params(60),
        cost_estimate=cost(2 * batch * width_dev * proj_width, 2 * width_dev * proj_width),
        name="project",
    )(tokens, attn_gain.reshape(1, width_dev), w_query, w_key, w_value, w_outgate, w_gates.T)
    state_short, w_output_near = pl.pallas_call(
        near_kernel,
        out_shape=(
            jax.ShapeDtypeStruct((rows * (value_size + 6), query_size), bf16),
            jax.ShapeDtypeStruct(w_output.shape, w_output.dtype),
        ),
        in_specs=[hbm] * 5,
        out_specs=[vmem] * 2,
        scratch_shapes=[
            pltpu.VMEM((rows, value_size, query_size), f32),
            pltpu.VMEM(state_n.shape, f32),
            pltpu.VMEM((1, rows), f32),
            pltpu.VMEM((1, heads_all), f32),
            pltpu.SemaphoreType.DMA((rows + 4,)),
        ],
        compiler_params=params(49),
        cost_estimate=cost(10**9, 6 * rows * value_size * query_size),
        name="near",
    )(
        state_c,
        w_output,
        state_n,
        state_m.reshape(1, rows),
        forget_bias.reshape(1, heads_all),
    )
    arrived = exchange(sent.reshape(kv_count, rows, proj_width + lanes), kv)
    head_copies, to_write, value = pl.pallas_call(
        functools.partial(cell_kernel, width_all, heads_all),
        out_shape=(
            jax.ShapeDtypeStruct((kv_count, rows, value_size), bf16),
            jax.ShapeDtypeStruct((rows, lanes + 2 * query_size), f32),
            jax.ShapeDtypeStruct((rows, value_size), f32),
        ),
        in_specs=[vmem] * 2,
        out_specs=[vmem] * 3,
        compiler_params=params(8),
        cost_estimate=cost(10**10, 4 * rows * value_size * query_size),
        name="cell",
    )(arrived, state_short)
    early_rows = rows // 4

    def written(first, count, extra, spec, scratch, *begun):
        return pl.pallas_call(
            functools.partial(write_kernel, first),
            out_shape=(jax.ShapeDtypeStruct(state_c.shape, f32), *extra),
            in_specs=[vmem, vmem, hbm] + [hbm] * len(begun),
            out_specs=(hbm,) + (spec,) * len(extra),
            input_output_aliases={3: 0} if begun else {},
            scratch_shapes=[
                pltpu.VMEM((count, value_size, query_size), f32),
                pltpu.SemaphoreType.DMA((count,)),
                pltpu.SemaphoreType.DMA((count + len(scratch),)),
                *scratch,
            ],
            compiler_params=params(50),
            cost_estimate=cost(10**9, 8 * count * value_size * query_size),
            name="write_state",
        )(to_write, value, state_c, *begun)

    begun_c, order = written(0, early_rows, (jax.ShapeDtypeStruct((8, lanes), f32),), vmem, ())
    new_c, new_n, new_m = written(
        early_rows,
        rows - early_rows,
        (jax.ShapeDtypeStruct(state_n.shape, f32), jax.ShapeDtypeStruct((1, rows), f32)),
        hbm,
        (pltpu.VMEM(state_n.shape, f32), pltpu.VMEM((1, rows), f32)),
        begun_c,
    )
    heads_rows = exchange(head_copies, kv).reshape(batch, value_size)
    attn_part = jnp.dot(heads_rows, w_output_near, preferred_element_type=f32)
    hidden_dev = w_gateff.shape[1]
    hidden_pad = -(-(hidden_dev + 2) // lanes) * lanes
    sent, middle = pl.pallas_call(
        widen_kernel,
        out_shape=(
            jax.ShapeDtypeStruct((batch, 2 * hidden_pad), bf16),
            jax.ShapeDtypeStruct((batch, width_dev), bf16),
        ),
        in_specs=[vmem] * 9,
        out_specs=[vmem] * 2,
        compiler_params=params(8),
        cost_estimate=cost(4 * batch * width_dev * hidden_dev, 4 * width_dev * hidden_dev),
        name="widen",
    )(
        *over_tp(attn_part),
        tokens,
        mlp_gain.reshape(1, width_dev),
        w_gateff.T,
        w_upff.T,
        order,
    )
    mid_float = middle.astype(f32)
    arrived = exchange(sent.reshape(kv_count, rows, 2 * hidden_pad), kv)
    hidden_copies = pl.pallas_call(
        functools.partial(hidden_kernel, width_all, hidden_dev),
        out_shape=jax.ShapeDtypeStruct((kv_count, rows, hidden_dev), bf16),
        in_specs=[vmem],
        out_specs=vmem,
        compiler_params=params(8),
        cost_estimate=cost(10**6, 4 * kv_count * rows * hidden_pad),
        name="hidden",
    )(arrived)
    hidden_rows = exchange(hidden_copies, kv).reshape(batch, hidden_dev)
    down_part = jnp.dot(hidden_rows, w_downff, preferred_element_type=jnp.float32)
    mixed = (mid_float + in_order(over_tp(down_part))).astype(jnp.bfloat16)
    return (mixed, new_c, new_n, new_m.reshape(rows, 1))


def solution(mesh):
    cores = 2
    tp_size = mesh.shape["tp"]
    fine = Mesh(
        mesh.devices.reshape(4, mesh.shape["kv"] // 4, tp_size // cores, cores), kv + tp
    )
    placed = (
        P(None, kv),
        P(kv),
        P(kv, tp),
        P(kv, tp),
        P(kv, tp),
        P(kv, tp),
        P(),
        P(),
        P(kv, tp, None, None),
        P(kv, tp, None),
        P(kv, tp),
        P(tp, kv),
        P(kv),
        P(kv, tp),
        P(kv, tp),
        P(tp, kv),
    )
    return jax.shard_map(
        per_device,
        mesh=fine,
        in_specs=placed,
        out_specs=(P(None, kv), P(kv, tp, None, None), P(kv, tp, None), P(kv, tp)),
        check_vma=False,
    )
```
